128 devices in a mesh: ep: 128 (over z, y, x, core).
Axes of the slice: x: 4, y: 4, z: 4, core: 2. Of those that a mesh axis runs over, the one named last changes fastest.
Arguments:
- residual: bfloat16 [8192, 2048], P('ep'), may hold values from -6 to 6
- branch_in: bfloat16 [8192, 1024], P('ep'), may hold values from -6 to 6
- state_real: float32 [8192, 4096], P('ep'), may hold values from -4 to 4
- state_imag: float32 [8192, 4096], P('ep'), may hold values from -4 to 4
- decay_rate: float32 [64, 64], replicated, may hold values from 0.1 to 1
- frequency: float32 [64, 64], replicated, may hold values from 0 to 200
- log_step: float32 [64], replicated, may hold values from -4 to 0
- input_real: bfloat16 [64, 64, 16], replicated, may hold values from -1 to 1
- input_imag: bfloat16 [64, 64, 16], replicated, may hold values from -1 to 1
- output_matrix_real: bfloat16 [64, 16, 64], replicated, may hold values from -0.5 to 0.5
- output_matrix_imaginary: bfloat16 [64, 16, 64], replicated, may hold values from -0.5 to 0.5
- skip_gain: float32 [1024], replicated, may hold values from -4 to 4
- glu_value: bfloat16 [1024, 2048], replicated, may hold values from -0.1875 to 0.1875
- glu_gate: bfloat16 [1024, 2048], replicated, may hold values from -0.1875 to 0.1875
- mix_gain: float32 [2048], replicated, may hold values from 0.1 to 1.9
- moe_in_gain: float32 [2048], replicated, may hold values from 0.1 to 1.9
- moe_out_gain: float32 [2048], replicated, may hold values from 0.1 to 1.9
- routes: int32 [8192, 6], P('ep'), may hold values from 0 to 127, all different within a row; in each aligned block of 64 rows (0 to 63, 64 to 127, ...) at most 4 rows name the same one
- route_weights: float32 [8192, 6], P('ep'), may hold values from 0.05 to 0.6
- expert_gate: bfloat16 [128, 2048, 512], P('ep'), may hold values from -0.125 to 0.125
- expert_up: bfloat16 [128, 2048, 512], P('ep'), may hold values from -0.125 to 0.125
- expert_down: bfloat16 [128, 512, 2048], P('ep'), may hold values from -0.25 to 0.25
- shared_gate: bfloat16 [2048, 512], replicated, may hold values from -0.125 to 0.125
- shared_up: bfloat16 [2048, 512], replicated, may hold values from -0.125 to 0.125
- shared_down: bfloat16 [512, 2048], replicated, may hold values from -0.25 to 0.25
Outputs:
- layer_out: bfloat16 [8192, 2048], P('ep')
- next_real: float32 [8192, 4096], P('ep')
- next_imag: float32 [8192, 4096], P('ep')
The draws below stay inside these ranges and needn't reach their ends.
Inputs may be any that keep to these rules, and one draw needn't show every extreme that they name: `routes`: among the rows of one device no expert is named more than 4 times, and in every draw some expert is named exactly 4 times by some device's rows; a token's experts are distinct.
All inputs are finite; a program needn't handle non-finite values.
Results may differ from the reference program's by a relative error of at most 0.0066.
Values may be sent and summed in bfloat16 or wider, within the bound.
No kernel may reach another device: no remote copies, remote signals or barrier semaphores. Data moves between devices by JAX's collectives and lax.ppermute only.
A program may use at most 128 MiB of HBM per device.

```python
import math
import jax
import jax.numpy as jnp
import numpy as np
from jax import lax

D = 2048
SSM_W = 1024
GCH = 16
GROUPS = 64
STATE = 64
EH = 512
TOP_K = 6
SEQ_DEV = 64
SEQS = 8192
EXPERTS = 128
CAP = 4
N_EP = 128


def levels(key, shape, pieces, least, largest):
    def one(dim, shards_of):
        steps = jax.random.uniform(jax.random.fold_in(jax.random.fold_in(key, 6), dim), (shards_of,), jnp.float32, least / len(pieces), largest / len(pieces))
        return jnp.repeat(jnp.exp(steps), shape[dim] // shards_of).reshape((-1,) + (1,) * (len(shape) - dim - 1))

    factor_of = one(*pieces[0])
    for cut in pieces[1:]:
        factor_of = factor_of * one(*cut)
    return factor_of


def shared_out(key, own, number, rows, amount, top, most, lean):
    ranking = jax.random.permutation(key, amount)
    heavy_load, ordinary = portions_of(amount, rows * top, most, lean, True), portions_of(amount, rows * top, most, lean, False)
    places = jnp.arange(amount)

    def named(sizes, rotation):
        used = int((sizes > 0).sum())
        fixed = max(1, used // 4)
        moved = fixed + (places - fixed + rotation * (used - fixed)) % max(1, amount - fixed)
        return jnp.zeros((amount,), jnp.int32).at[ranking[jnp.where(places < fixed, places, moved)]].set(jnp.asarray(sizes, jnp.int32))

    sizes = jnp.where(number % 4 == 0, named(heavy_load, number // 4), named(ordinary, number - number // 4 - 1))
    mixed = jax.random.permutation(jax.random.fold_in(own, 3), amount)
    source_of, sink = mixed[0:amount // 2 * 2:2], mixed[1:amount // 2 * 2:2]
    slack = jnp.minimum(sizes[source_of] - 1, most - sizes[sink]) // 2
    slack = jnp.where((source_of == ranking[0]) | (sink == ranking[0]) | (sizes[sink] == 0), 0, jnp.maximum(slack, 0))
    moved = jax.random.randint(jax.random.fold_in(own, 4), (amount // 2,), 0, 1 << 20) % (slack + 1)
    sizes = sizes.at[source_of].add(-moved).at[sink].add(moved)
    items = jnp.searchsorted(jnp.cumsum(sizes), jnp.arange(rows * top), side="right").astype(jnp.int32)
    table = items.reshape(top, rows).T
    table = table[jax.random.permutation(jax.random.fold_in(own, 1), rows)]
    rotation = jax.random.randint(jax.random.fold_in(own, 2), (rows, 1), 0, top)
    return jnp.take_along_axis(table, (jnp.arange(top)[None, :] + rotation) % top, axis=1)


def portions_of(amount, total, reach, skew, full):
    weights = [(1 << 20) // math.isqrt(rank ** skew) + 1 for rank in range(1, amount + 1)]
    largest = reach if full else min(reach, max(-(-total // amount), total * weights[0] // sum(weights)))
    least = 1 if total - largest >= amount - 1 else 0
    given, surplus = [largest] + [least] * (amount - 1), total - largest - least * (amount - 1)
    while surplus > 0:
        candidates = [i for i in range(1, amount) if given[i] < largest] or [i for i in range(1, amount) if given[i] < reach]
        whole, left = sum([weights[i] for i in candidates]), surplus
        for i in candidates:
            more = min(reach - given[i], max(1, left * weights[i] // whole), surplus)
            given[i] = given[i] + more
            surplus = surplus - more
    return np.array(given)


def bell_draw(rng, shape, deviation, reach, split=(), kind=jnp.bfloat16):
    loudness = levels(rng, shape, split, -0.22, 0.18) if split else 1.0
    array = jax.random.normal(rng, shape, jnp.float32) * deviation * loudness
    return jnp.minimum(jnp.maximum(array, -reach), reach).astype(kind)


def setup_inputs(seed: int = 0) -> dict:
    arg_keys = jax.random.split(jax.random.key(seed), 26)
    residual = bell_draw(arg_keys[0], (SEQS, D), 1.0, 6.0, ((0, 128),))
    branch_in = bell_draw(arg_keys[1], (SEQS, SSM_W), 1.0, 6.0, ((0, 128),))
    state_real = bell_draw(arg_keys[2], (SEQS, GROUPS * STATE), 0.5, 4.0, ((0, 128),), jnp.float32)
    state_imag = bell_draw(arg_keys[3], (SEQS, GROUPS * STATE), 0.5, 4.0, ((0, 128),), jnp.float32)
    decay_rate = jnp.clip(jnp.exp(jax.random.uniform(arg_keys[4], (GROUPS, STATE), jnp.float32, math.log(0.1), math.log(1.0))), 0.1, 1.0)
    frequency = jnp.clip(jax.random.uniform(arg_keys[5], (GROUPS, STATE), jnp.float32, 0.0, 200.0), 0.0, 200.0)
    log_step = jnp.clip(jax.random.uniform(arg_keys[6], (GROUPS,), jnp.float32, -4.0, 0.0), -4.0, 0.0)
    input_real = bell_draw(arg_keys[7], (GROUPS, STATE, GCH), (2 * GCH) ** -0.5, 1.0)
    input_imag = bell_draw(arg_keys[8], (GROUPS, STATE, GCH), (2 * GCH) ** -0.5, 1.0)
    output_matrix_real = bell_draw(arg_keys[9], (GROUPS, GCH, STATE), (2 * STATE) ** -0.5, 0.5)
    output_matrix_imaginary = bell_draw(arg_keys[10], (GROUPS, GCH, STATE), (2 * STATE) ** -0.5, 0.5)
    skip_gain = bell_draw(arg_keys[11], (SSM_W,), 1.0, 4.0, (), jnp.float32)
    glu_value = bell_draw(arg_keys[12], (SSM_W, D), SSM_W ** -0.5, 0.1875)
    glu_gate = bell_draw(arg_keys[13], (SSM_W, D), SSM_W ** -0.5, 0.1875)
    mix_gain = jnp.clip(1.0 + 0.18 * jax.random.normal(arg_keys[14], (D,), jnp.float32), 0.1, 1.9)
    moe_in_gain = jnp.clip(1.0 + 0.18 * jax.random.normal(arg_keys[15], (D,), jnp.float32), 0.1, 1.9)
    moe_out_gain = jnp.clip(1.0 + 0.18 * jax.random.normal(arg_keys[16], (D,), jnp.float32), 0.1, 1.9)
    routes_keys = jax.random.split(jax.random.fold_in(arg_keys[17], 1), SEQS // SEQ_DEV)
    routes_turns = jax.random.permutation(jax.random.fold_in(arg_keys[17], 3), SEQS // SEQ_DEV)
    routes = jax.vmap(lambda own, number: shared_out(jax.random.fold_in(arg_keys[17], 2), own, number, SEQ_DEV, EXPERTS, TOP_K, CAP, 2))(routes_keys, routes_turns).reshape((SEQS, TOP_K))
    route_weights = jnp.clip(0.05 + 0.55 * jax.random.uniform(arg_keys[18], (SEQS, TOP_K), jnp.float32) ** levels(arg_keys[18], (SEQS, TOP_K), ((0, 128),), -0.2, 0.2), 0.05, 0.6)
    expert_gate = bell_draw(arg_keys[19], (EXPERTS, D, EH), D ** -0.5, 0.125, ((0, 128),))
    expert_up = bell_draw(arg_keys[20], (EXPERTS, D, EH), D ** -0.5, 0.125, ((0, 128),))
    expert_down = bell_draw(arg_keys[21], (EXPERTS, EH, D), EH ** -0.5, 0.25, ((0, 128),))
    shared_gate = bell_draw(arg_keys[22], (D, EH), D ** -0.5, 0.125)
    shared_up = bell_draw(arg_keys[23], (D, EH), D ** -0.5, 0.125)
    shared_down = bell_draw(arg_keys[24], (EH, D), EH ** -0.5, 0.25)
    return dict(residual=residual, branch_in=branch_in, state_real=state_real, state_imag=state_imag, decay_rate=decay_rate, frequency=frequency, log_step=log_step, input_real=input_real, input_imag=input_imag, output_matrix_real=output_matrix_real, output_matrix_imaginary=output_matrix_imaginary, skip_gain=skip_gain, glu_value=glu_value, glu_gate=glu_gate, mix_gain=mix_gain, moe_in_gain=moe_in_gain, moe_out_gain=moe_out_gain, routes=routes, route_weights=route_weights, expert_gate=expert_gate, expert_up=expert_up, expert_down=expert_down, shared_gate=shared_gate, shared_up=shared_up, shared_down=shared_down)


norm_eps = 1e-06

def scaled_norm(row_block, norm_gain):
    return row_block * lax.rsqrt(lax.optimization_barrier(jnp.mean(row_block * row_block, axis=-1, keepdims=True)) + norm_eps) * norm_gain

def state_step(branch_in, state_real, state_imag, decay_rate, frequency, log_step, input_real, input_imag, output_matrix_real, output_matrix_imaginary, skip_gain):
    seq_count = branch_in.shape[0]
    group_count, state_count = decay_rate.shape
    chan_count = input_real.shape[2]
    step_size = jnp.exp(log_step)[:, None]
    magnitude = jnp.exp(-decay_rate * step_size)
    abar_re = magnitude * jnp.cos(frequency * step_size)
    abar_im = magnitude * jnp.sin(frequency * step_size)
    lam_re = -decay_rate
    lam_im = frequency
    denominator = lam_re * lam_re + lam_im * lam_im
    numer_re = abar_re - 1.0
    coef_re = (numer_re * lam_re + abar_im * lam_im) / denominator
    coef_im = (abar_im * lam_re - numer_re * lam_im) / denominator
    b_real = input_real.astype(jnp.float32)
    b_imag = input_imag.astype(jnp.float32)
    bbar_re = coef_re[..., None] * b_real - coef_im[..., None] * b_imag
    bbar_im = coef_re[..., None] * b_imag + coef_im[..., None] * b_real
    feed_rows = branch_in.astype(jnp.float32).reshape(seq_count, group_count, chan_count)
    forcing_real = jnp.einsum('tgc,gpc->tgp', feed_rows, bbar_re, precision=lax.Precision.HIGHEST)
    drive_im = jnp.einsum('tgc,gpc->tgp', feed_rows, bbar_im, precision=lax.Precision.HIGHEST)
    old_re = state_real.reshape(seq_count, group_count, state_count)
    old_im = state_imag.reshape(seq_count, group_count, state_count)
    fresh_real = abar_re * old_re - abar_im * old_im + forcing_real
    fresh_imaginary = abar_re * old_im + abar_im * old_re + drive_im
    state_readout = jnp.einsum('ukb,krb->ukr', fresh_real, output_matrix_real.astype(jnp.float32), precision=lax.Precision.HIGHEST) - jnp.einsum('ukb,krb->ukr', fresh_imaginary, output_matrix_imaginary.astype(jnp.float32), precision=lax.Precision.HIGHEST)
    mixed_rows = state_readout.reshape(seq_count, group_count * chan_count) + skip_gain * branch_in.astype(jnp.float32)
    activated = jax.nn.gelu(mixed_rows).astype(jnp.bfloat16)
    return (activated, fresh_real.reshape(seq_count, -1), fresh_imaginary.reshape(seq_count, -1))

def expert_rows(row_block, w_gate, w_up, w_down):
    gate_part = jnp.dot(row_block, w_gate, preferred_element_type=jnp.float32)
    up_part = jnp.dot(row_block, w_up, preferred_element_type=jnp.float32)
    hidden = (jax.nn.silu(gate_part) * up_part).astype(jnp.bfloat16)
    return jnp.dot(hidden, w_down, preferred_element_type=jnp.float32)

def mixer_residual(residual, activated, glu_value, glu_gate, mix_gain):
    value_part = jnp.dot(activated, glu_value, preferred_element_type=jnp.float32)
    gate_part = jnp.dot(activated, glu_gate, preferred_element_type=jnp.float32)
    branch = value_part * jax.nn.sigmoid(gate_part)
    return (residual.astype(jnp.float32) + scaled_norm(branch, mix_gain)).astype(jnp.bfloat16)

def reference(residual, branch_in, state_real, state_imag, decay_rate, frequency, log_step, input_real, input_imag, output_matrix_real, output_matrix_imaginary, skip_gain, glu_value, glu_gate, mix_gain, moe_in_gain, moe_out_gain, routes, route_weights, expert_gate, expert_up, expert_down, shared_gate, shared_up, shared_down):
    activated, next_real, next_imag = state_step(branch_in, state_real, state_imag, decay_rate, frequency, log_step, input_real, input_imag, output_matrix_real, output_matrix_imaginary, skip_gain)
    resid_mid = mixer_residual(residual, activated, glu_value, glu_gate, mix_gain)
    normed = scaled_norm(resid_mid.astype(jnp.float32), moe_in_gain).astype(jnp.bfloat16)
    hidden_width = normed.shape[1]
    flat_routes = routes.reshape(-1).astype(jnp.int32)
    assign_count = flat_routes.shape[0]
    sorted_order = jnp.argsort(flat_routes, stable=True).astype(jnp.int32)
    sorted_expert = flat_routes[sorted_order]
    expert_load = lax.optimization_barrier(jnp.sum((flat_routes[:, None] == jnp.arange(EXPERTS, dtype=jnp.int32)[None, :]).astype(jnp.int32), axis=0))
    load_start = jnp.cumsum(expert_load) - expert_load
    slot_rank = jnp.arange(assign_count, dtype=jnp.int32) - load_start[sorted_expert]
    slot_most = CAP * N_EP
    slot_index = (sorted_expert * slot_most + slot_rank).astype(jnp.int32)
    slot_table = jnp.full((EXPERTS * slot_most,), SEQS, jnp.int32).at[slot_index].set(sorted_order // TOP_K)
    padded = jnp.concatenate([normed, jnp.zeros((1, hidden_width), jnp.bfloat16)], axis=0)

    def one_expert(expert_args):
        row_ids, w_gate, w_up, w_down = expert_args
        return expert_rows(padded[row_ids], w_gate, w_up, w_down).astype(jnp.bfloat16)
    expert_out = lax.map(one_expert, (slot_table.reshape(EXPERTS, slot_most), expert_gate, expert_up, expert_down))
    assign_slot = jnp.zeros((assign_count,), jnp.int32).at[sorted_order].set(slot_index)
    per_assign = expert_out.reshape(-1, hidden_width)[assign_slot].reshape(SEQS, TOP_K, hidden_width).astype(jnp.float32)
    routed = lax.optimization_barrier(jnp.sum(per_assign * route_weights[..., None], axis=1))
    shared = expert_rows(normed, shared_gate, shared_up, shared_down)
    combined = shared + routed
    layer_out = (resid_mid.astype(jnp.float32) + scaled_norm(combined, moe_out_gain)).astype(jnp.bfloat16)
    return (layer_out, next_real, next_imag)
```

```python
import functools

import jax
import jax.numpy as jnp
from jax import lax
from jax.experimental import pallas as pl
from jax.experimental.pallas import tpu as pltpu
from jax.sharding import PartitionSpec as P

norm_eps = 1e-06
f32 = jnp.float32
bf16 = jnp.bfloat16

CHUNK = 256
CAPACITY = 4
PARTS = 4


def iota(shape, dim):
    return lax.broadcasted_iota(jnp.int32, shape, dim)


def dot(a, b):
    return jnp.dot(a, b, preferred_element_type=f32)


def sin_cos(x):
    turns = jnp.floor(x * 0.6366197723675814 + 0.5)
    r = ((x - turns * 1.5703125) - turns * 4.837512969970703125e-4) - turns * 7.54978995489188216e-8
    z = r * r
    s = r + r * z * ((-1.9515295891e-4 * z + 8.3321608736e-3) * z - 1.6666654611e-1)
    c = 1.0 - 0.5 * z + z * z * (
        (2.443315711809948e-5 * z - 1.388731625493765e-3) * z + 4.166664568298827e-2
    )
    quarter = turns.astype(jnp.int32) & 3
    odd = (quarter & 1) == 1
    sin_x = jnp.where(odd, c, s)
    cos_x = jnp.where(odd, s, c)
    sin_x = jnp.where(quarter >= 2, -sin_x, sin_x)
    cos_x = jnp.where((quarter == 1) | (quarter == 2), -cos_x, cos_x)
    return sin_x, cos_x


def split(x):
    hi = x.astype(bf16)
    return hi, (x - hi.astype(f32)).astype(bf16)


def route_code(routes):
    top, seq = routes.shape
    experts = 128
    row = iota((experts, seq), 0)
    named = jnp.zeros((experts, seq), f32)
    for k in range(top):
        named = named + jnp.where(row == routes[k : k + 1, :], 1.0, 0.0)
    before = jnp.where(iota((seq, seq), 0) < iota((seq, seq), 1), 1.0, 0.0).astype(bf16)
    rank = dot(named.astype(bf16), before)
    return jnp.where(named > 0.5, rank, -1.0)


def spread_rows(block):
    one_hot = jnp.where(iota((CHUNK, 16), 0) // 16 == iota((CHUNK, 16), 1), 1.0, 0.0)
    return dot(one_hot.astype(bf16), block.astype(bf16))


def slot_pattern(seq):
    i = iota((CHUNK, PARTS * seq), 0)
    j = iota((CHUNK, PARTS * seq), 1)
    return jnp.where((i // 4) % 4 == j // seq, (i % 4).astype(f32), -2.0)


def rms_scale(x):
    return lax.rsqrt(jnp.mean(x * x, axis=-1, keepdims=True) + norm_eps)


def mixer_kernel(
    u_ref, sr_ref, si_ref, decay_ref, freq_ref, log_ref, inr_ref, ini_ref, cr_ref, ci_ref,
    skip_ref, gv_ref, gg_ref, res_ref, mix_ref, gain_ref, routes_ref,
    nr_ref, ni_ref, mid_ref, normed_ref, out_ref,
    br, bi, cr, ci, acc_v, acc_g,
):
    step = pl.program_id(0)
    groups, states = decay_ref.shape
    chans = inr_ref.shape[0] // groups
    seq = u_ref.shape[0]
    wide = groups * states

    @pl.when(step == 0)
    def _():
        for ref in (br, bi, cr, ci):
            ref[...] = jnp.zeros_like(ref)
        acc_v[...] = jnp.zeros_like(acc_v)
        acc_g[...] = jnp.zeros_like(acc_g)

    logs = log_ref[...]
    pick = iota((groups, logs.shape[1]), 1) == iota((groups, logs.shape[1]), 0) + step * groups
    step_size = jnp.exp(jnp.sum(jnp.where(pick, logs, 0.0), axis=1, keepdims=True))
    decay = decay_ref[...]
    freq = freq_ref[...]
    magnitude = jnp.exp(-decay * step_size)
    sin_x, cos_x = sin_cos(freq * step_size)
    a_re = magnitude * cos_x
    a_im = magnitude * sin_x
    lam = -decay
    den = lam * lam + freq * freq
    num = a_re - 1.0
    k_re = (num * lam + a_im * freq) / den
    k_im = (a_im * lam - num * freq) / den

    lane_group = iota((groups, wide), 1) // states
    own = iota((groups, wide), 0) == lane_group

    def flat(x):
        twice = jnp.concatenate([x, x], axis=1)
        tiled = jnp.concatenate([twice] * (groups // 2), axis=1)
        return jnp.sum(jnp.where(own, tiled, 0.0), axis=0, keepdims=True)

    a_re, a_im, k_re, k_im = flat(a_re), flat(a_im), flat(k_re), flat(k_im)

    rows = groups * chans
    patch = (iota((rows, 2 * states), 0) // chans) % 2 == iota((rows, 2 * states), 1) // states
    for ref, src in ((br, inr_ref), (bi, ini_ref), (cr, cr_ref), (ci, ci_ref)):
        x = src[...].astype(f32)
        x = jnp.where(patch, jnp.concatenate([x, x], axis=1), 0.0).astype(bf16)
        for j in range(groups // 2):
            r = slice(2 * chans * j, 2 * chans * (j + 1))
            ref[r, 2 * states * j : 2 * states * (j + 1)] = x[r]

    u = u_ref[...]
    f_re = dot(u, br[...])
    f_im = dot(u, bi[...])
    old_re = sr_ref[...]
    old_im = si_ref[...]
    new_re = a_re * old_re - a_im * old_im + (k_re * f_re - k_im * f_im)
    new_im = a_re * old_im + a_im * old_re + (k_re * f_im + k_im * f_re)
    nr_ref[...] = new_re
    ni_ref[...] = new_im

    def read(x, m):
        hi, lo = split(x)
        both = lax.dot_general(
            jnp.concatenate([hi, lo], axis=0), m, (((1,), (1,)), ((), ())),
            preferred_element_type=f32,
        )
        return both[:seq] + both[seq:]

    mixed = read(new_re, cr[...]) - read(new_im, ci[...]) + skip_ref[...] * u.astype(f32)
    act = jax.nn.gelu(mixed).astype(bf16)
    acc_v[...] += dot(act, gv_ref[...])
    acc_g[...] += dot(act, gg_ref[...])

    @pl.when(step == pl.num_programs(0) - 1)
    def _():
        branch = acc_v[...] * jax.nn.sigmoid(acc_g[...])
        mid = (res_ref[...].astype(f32) + branch * rms_scale(branch) * mix_ref[...]).astype(bf16)
        mid_ref[...] = mid
        mid = mid.astype(f32)
        normed = (mid * rms_scale(mid) * gain_ref[...]).astype(bf16)
        normed_ref[...] = normed
        part = normed.shape[1] // PARTS
        stacked = jnp.concatenate(
            [normed[:, part * q : part * (q + 1)] for q in range(PARTS)], axis=0
        )
        code = route_code(routes_ref[...])
        code = jnp.concatenate([code] * PARTS, axis=1)
        want = slot_pattern(seq)
        for c in range(out_ref.shape[0] // CHUNK):
            here = spread_rows(code[16 * c : 16 * (c + 1)])
            select = jnp.where(here == want, 1.0, 0.0).astype(bf16)
            out_ref[CHUNK * c : CHUNK * (c + 1), :] = dot(select, stacked).astype(bf16)


def run_mixer(
    u, sr, si, decay, freq, log_step, inr, ini, cr, ci, skip, gv, gg, res, mix, gain, routes
):
    seq, width = u.shape
    model = res.shape[1]
    steps = 4
    groups, states = decay.shape
    part = model // PARTS
    gb, cb, wb = groups // steps, width // steps, groups * states // steps
    cols = lambda n: pl.BlockSpec((seq, n), lambda i: (0, i))
    rows = lambda r, n: pl.BlockSpec((r, n), lambda i: (i, 0))
    whole = lambda x: pl.BlockSpec(x.shape, lambda i: (0, 0))
    out_rows = 128 * CAPACITY * PARTS
    return pl.pallas_call(
        mixer_kernel,
        grid=(steps,),
        in_specs=[
            cols(cb), cols(wb), cols(wb), rows(gb, states), rows(gb, states), whole(log_step),
            rows(cb, states), rows(cb, states), rows(cb, states), rows(cb, states),
            pl.BlockSpec((1, cb), lambda i: (0, i)),
            rows(cb, model), rows(cb, model), whole(res), whole(mix), whole(gain), whole(routes),
        ],
        out_specs=[
            cols(wb), cols(wb),
            pl.BlockSpec((seq, model), lambda i: (0, 0)),
            pl.BlockSpec((seq, model), lambda i: (0, 0)),
            pl.BlockSpec((out_rows, part), lambda i: (0, 0)),
        ],
        out_shape=[
            jax.ShapeDtypeStruct(sr.shape, f32),
            jax.ShapeDtypeStruct(si.shape, f32),
            jax.ShapeDtypeStruct((seq, model), bf16),
            jax.ShapeDtypeStruct((seq, model), bf16),
            jax.ShapeDtypeStruct((out_rows, part), bf16),
        ],
        scratch_shapes=[pltpu.VMEM((cb, wb), bf16)] * 4 + [pltpu.VMEM((seq, model), f32)] * 2,
        name="mixer",
    )(u, sr, si, decay, freq, log_step, inr, ini, cr, ci, skip, gv, gg, res, mix, gain, routes)


def swap_matrix(back):
    i = iota((CHUNK, CHUNK), 1 if back else 0)
    j = iota((CHUNK, CHUNK), 0 if back else 1)
    source = ((i // 4) % 16) * 16 + (i // 64) * 4 + i % 4
    return jnp.where(source == j, 1.0, 0.0).astype(bf16)


def expert_kernel(y_ref, wg_ref, wu_ref, wd_ref, z_ref):
    model = wg_ref.shape[0]
    part = model // PARTS
    take = CHUNK // PARTS
    order = swap_matrix(False)
    pieces = []
    for c in range(y_ref.shape[0] // CHUNK):
        x = dot(order, y_ref[CHUNK * c : CHUNK * (c + 1), :]).astype(bf16)
        pieces.append(
            jnp.concatenate([x[take * q : take * (q + 1)] for q in range(PARTS)], axis=1)
        )
    x = jnp.concatenate(pieces, axis=0)
    gate = dot(x, wg_ref[...])
    up = dot(x, wu_ref[...])
    hidden = (gate * jax.nn.sigmoid(gate) * up).astype(bf16)
    out = dot(hidden, wd_ref[...]).astype(bf16)
    back = swap_matrix(True)
    for c in range(y_ref.shape[0] // CHUNK):
        o = out[take * c : take * (c + 1)]
        o = jnp.concatenate([o[:, part * q : part * (q + 1)] for q in range(PARTS)], axis=0)
        z_ref[CHUNK * c : CHUNK * (c + 1), :] = dot(back, o).astype(bf16)


def run_expert(y, wg, wu, wd):
    steps = 4
    whole = lambda x: pl.BlockSpec(x.shape, lambda i: (0, 0))
    block = pl.BlockSpec((y.shape[0] // steps, y.shape[1]), lambda i: (i, 0))
    return pl.pallas_call(
        expert_kernel,
        grid=(steps,),
        in_specs=[block, whole(wg), whole(wu), whole(wd)],
        out_specs=block,
        out_shape=jax.ShapeDtypeStruct(y.shape, bf16),
        name="expert",
    )(y, wg, wu, wd)


def shared_kernel(normed_ref, wg_ref, wu_ref, wd_ref, routes_ref, weights_ref, out_ref, mix_ref):
    x = normed_ref[...]
    gate = dot(x, wg_ref[...])
    up = dot(x, wu_ref[...])
    hidden = (gate * jax.nn.sigmoid(gate) * up).astype(bf16)
    out_ref[...] = dot(hidden, wd_ref[...])

    routes = routes_ref[...]
    weights = weights_ref[...]
    top, seq = routes.shape
    code = route_code(routes)
    row = iota(code.shape, 0)
    weight = jnp.zeros(code.shape, f32)
    for k in range(top):
        weight = weight + jnp.where(row == routes[k : k + 1, :], weights[k : k + 1, :], 0.0)
    code = jnp.concatenate([code] * PARTS, axis=1)
    weight = jnp.concatenate([weight] * PARTS, axis=1)
    hi, lo = split(weight)
    want = slot_pattern(seq)
    for c in range(mix_ref.shape[0] // CHUNK):
        r = slice(16 * c, 16 * (c + 1))
        hit = spread_rows(code[r]) == want
        for h, w in enumerate((hi, lo)):
            mix_ref[CHUNK * c : CHUNK * (c + 1), PARTS * seq * h : PARTS * seq * (h + 1)] = (
                jnp.where(hit, spread_rows(w[r]), 0.0).astype(bf16)
            )


def run_shared(normed, wg, wu, wd, routes, weights):
    seq, model = normed.shape
    return pl.pallas_call(
        shared_kernel,
        out_shape=[
            jax.ShapeDtypeStruct((seq, model), f32),
            jax.ShapeDtypeStruct((128 * CAPACITY * PARTS, 2 * PARTS * seq), bf16),
        ],
        cost_estimate=pl.CostEstimate(
            flops=2 * seq * model * wg.shape[1] * 60, bytes_accessed=8 << 20, transcendentals=0
        ),
        name="shared",
    )(normed, wg, wu, wd, routes, weights)


def combine_kernel(z_ref, mix_ref, shared_ref, mid_ref, gain_ref, out_ref):
    seq = mid_ref.shape[0]
    both = lax.dot_general(
        mix_ref[...], z_ref[...], (((0,), (0,)), ((), ())), preferred_element_type=f32
    )
    both = both[: PARTS * seq] + both[PARTS * seq :]
    routed = jnp.concatenate([both[seq * q : seq * (q + 1)] for q in range(PARTS)], axis=1)
    combined = shared_ref[...] + routed
    out_ref[...] = (
        mid_ref[...].astype(f32) + combined * rms_scale(combined) * gain_ref[...]
    ).astype(bf16)


def run_combine(z, mix, shared, mid, gain):
    return pl.pallas_call(
        combine_kernel,
        out_shape=jax.ShapeDtypeStruct(mid.shape, bf16),
        name="combine",
    )(z, mix, shared, mid, gain)


def per_device(
    residual, branch_in, state_real, state_imag, decay_rate, frequency, log_step, input_real,
    input_imag, output_matrix_real, output_matrix_imaginary, skip_gain, glu_value, glu_gate,
    mix_gain, moe_in_gain, moe_out_gain, routes, route_weights, expert_gate, expert_up,
    expert_down, shared_gate, shared_up, shared_down,
):
    states = decay_rate.shape[1]
    model = residual.shape[1]
    part = model // PARTS
    row = lambda v: v.reshape(1, -1)
    inr = jnp.transpose(input_real, (0, 2, 1)).reshape(-1, states)
    ini = jnp.transpose(input_imag, (0, 2, 1)).reshape(-1, states)
    cr = output_matrix_real.reshape(-1, states)
    ci = output_matrix_imaginary.reshape(-1, states)
    routes_t = routes.T
    weights_t = route_weights.T
    next_real, next_imag, mid, normed, outgoing = run_mixer(
        branch_in, state_real, state_imag, decay_rate, frequency, row(log_step), inr, ini, cr, ci,
        row(skip_gain), glu_value, glu_gate, residual, row(mix_gain), row(moe_in_gain), routes_t,
    )

    def exchange(x):
        x = x.reshape(128, PARTS * CAPACITY, part)
        return lax.all_to_all(x, "ep", split_axis=0, concat_axis=0, tiled=True).reshape(-1, part)

    arrived = exchange(outgoing)
    shared, mix = run_shared(normed, shared_gate, shared_up, shared_down, routes_t, weights_t)
    returned = exchange(run_expert(arrived, expert_gate[0], expert_up[0], expert_down[0]))
    layer_out = run_combine(returned, mix, shared, mid, row(moe_out_gain))
    return layer_out, next_real, next_imag


def solution(mesh):
    rows2 = P("ep", None)
    rows3 = P("ep", None, None)
    return jax.shard_map(
        per_device,
        mesh=mesh,
        in_specs=(rows2,) * 4 + (P(),) * 13 + (rows2,) * 2 + (rows3,) * 3 + (P(),) * 3,
        out_specs=(rows2, rows2, rows2),
        check_vma=False,
    )
```

```python
import functools

import jax
import jax.numpy as jnp
from jax import lax
from jax.experimental import pallas as pl
from jax.experimental.pallas import tpu as pltpu
from jax.sharding import PartitionSpec as P

norm_eps = 1e-06
f32 = jnp.float32
bf16 = jnp.bfloat16

CHUNK = 256
CAPACITY = 4
PARTS = 4


def iota(shape, dim):
    return lax.broadcasted_iota(jnp.int32, shape, dim)


def dot(a, b):
    return jnp.dot(a, b, preferred_element_type=f32)


def sin_cos(x):
    turns = jnp.floor(x * 0.6366197723675814 + 0.5)
    r = ((x - turns * 1.5703125) - turns * 4.837512969970703125e-4) - turns * 7.54978995489188216e-8
    z = r * r
    s = r + r * z * ((-1.9515295891e-4 * z + 8.3321608736e-3) * z - 1.6666654611e-1)
    c = 1.0 - 0.5 * z + z * z * (
        (2.443315711809948e-5 * z - 1.388731625493765e-3) * z + 4.166664568298827e-2
    )
    quarter = turns.astype(jnp.int32) & 3
    odd = (quarter & 1) == 1
    sin_x = jnp.where(odd, c, s)
    cos_x = jnp.where(odd, s, c)
    sin_x = jnp.where(quarter >= 2, -sin_x, sin_x)
    cos_x = jnp.where((quarter == 1) | (quarter == 2), -cos_x, cos_x)
    return sin_x, cos_x


def split(x):
    hi = x.astype(bf16)
    return hi, (x - hi.astype(f32)).astype(bf16)


def route_code(routes):
    top, seq = routes.shape
    experts = 128
    row = iota((experts, seq), 0)
    named = jnp.zeros((experts, seq), f32)
    for k in range(top):
        named = named + jnp.where(row == routes[k : k + 1, :], 1.0, 0.0)
    before = jnp.where(iota((seq, seq), 0) < iota((seq, seq), 1), 1.0, 0.0).astype(bf16)
    rank = dot(named.astype(bf16), before)
    return jnp.where(named > 0.5, rank, -1.0)


def spread_rows(block):
    one_hot = jnp.where(iota((CHUNK, 16), 0) // 16 == iota((CHUNK, 16), 1), 1.0, 0.0)
    return dot(one_hot.astype(bf16), block.astype(bf16))


def slot_pattern(seq):
    i = iota((CHUNK, PARTS * seq), 0)
    j = iota((CHUNK, PARTS * seq), 1)
    return jnp.where((i // 4) % 4 == j // seq, (i % 4).astype(f32), -2.0)


def rms_scale(x):
    return lax.rsqrt(jnp.mean(x * x, axis=-1, keepdims=True) + norm_eps)


def mixer_kernel(
    u_ref, sr_ref, si_ref, decay_ref, freq_ref, log_ref, inr_ref, ini_ref, cr_ref, ci_ref,
    skip_ref, gv_ref, gg_ref, res_ref, mix_ref, gain_ref, routes_ref,
    nr_ref, ni_ref, mid_ref, normed_ref, out_ref,
    br, bi, cr, ci, acc_v, acc_g,
):
    step = pl.program_id(0)
    groups, states = decay_ref.shape
    chans = inr_ref.shape[0] // groups
    seq = u_ref.shape[0]
    wide = groups * states

    @pl.when(step == 0)
    def _():
        for ref in (br, bi, cr, ci):
            ref[...] = jnp.zeros_like(ref)
        acc_v[...] = jnp.zeros_like(acc_v)
        acc_g[...] = jnp.zeros_like(acc_g)

    logs = log_ref[...]
    pick = iota((groups, logs.shape[1]), 1) == iota((groups, logs.shape[1]), 0) + step * groups
    step_size = jnp.exp(jnp.sum(jnp.where(pick, logs, 0.0), axis=1, keepdims=True))
    decay = decay_ref[...]
    freq = freq_ref[...]
    magnitude = jnp.exp(-decay * step_size)
    sin_x, cos_x = sin_cos(freq * step_size)
    a_re = magnitude * cos_x
    a_im = magnitude * sin_x
    lam = -decay
    den = lam * lam + freq * freq
    num = a_re - 1.0
    k_re = (num * lam + a_im * freq) / den
    k_im = (a_im * lam - num * freq) / den

    lane_group = iota((groups, wide), 1) // states
    own = iota((groups, wide), 0) == lane_group

    def flat(x):
        twice = jnp.concatenate([x, x], axis=1)
        tiled = jnp.concatenate([twice] * (groups // 2), axis=1)
        return jnp.sum(jnp.where(own, tiled, 0.0), axis=0, keepdims=True)

    a_re, a_im, k_re, k_im = flat(a_re), flat(a_im), flat(k_re), flat(k_im)

    rows = groups * chans
    patch = (iota((rows, 2 * states), 0) // chans) % 2 == iota((rows, 2 * states), 1) // states
    for ref, src in ((br, inr_ref), (bi, ini_ref), (cr, cr_ref), (ci, ci_ref)):
        x = src[...].astype(f32)
        x = jnp.where(patch, jnp.concatenate([x, x], axis=1), 0.0).astype(bf16)
        for j in range(groups // 2):
            r = slice(2 * chans * j, 2 * chans * (j + 1))
            ref[r, 2 * states * j : 2 * states * (j + 1)] = x[r]

    u = u_ref[...]
    f_re = dot(u, br[...])
    f_im = dot(u, bi[...])
    old_re = sr_ref[...]
    old_im = si_ref[...]
    new_re = a_re * old_re - a_im * old_im + (k_re * f_re - k_im * f_im)
    new_im = a_re * old_im + a_im * old_re + (k_re * f_im + k_im * f_re)
    nr_ref[...] = new_re
    ni_ref[...] = new_im

    def read(x, m):
        hi, lo = split(x)
        both = lax.dot_general(
            jnp.concatenate([hi, lo], axis=0), m, (((1,), (1,)), ((), ())),
            preferred_element_type=f32,
        )
        return both[:seq] + both[seq:]

    mixed = read(new_re, cr[...]) - read(new_im, ci[...]) + skip_ref[...] * u.astype(f32)
    act = jax.nn.gelu(mixed).astype(bf16)
    acc_v[...] += dot(act, gv_ref[...])
    acc_g[...] += dot(act, gg_ref[...])

    @pl.when(step == pl.num_programs(0) - 1)
    def _():
        branch = acc_v[...] * jax.nn.sigmoid(acc_g[...])
        mid = (res_ref[...].astype(f32) + branch * rms_scale(branch) * mix_ref[...]).astype(bf16)
        mid_ref[...] = mid
        mid = mid.astype(f32)
        normed = (mid * rms_scale(mid) * gain_ref[...]).astype(bf16)
        normed_ref[...] = normed
        part = normed.shape[1] // PARTS
        stacked = jnp.concatenate(
            [normed[:, part * q : part * (q + 1)] for q in range(PARTS)], axis=0
        )
        code = route_code(routes_ref[...])
        code = jnp.concatenate([code] * PARTS, axis=1)
        want = slot_pattern(seq)
        for c in range(out_ref.shape[0] // CHUNK):
            here = spread_rows(code[16 * c : 16 * (c + 1)])
            select = jnp.where(here == want, 1.0, 0.0).astype(bf16)
            out_ref[CHUNK * c : CHUNK * (c + 1), :] = dot(select, stacked).astype(bf16)


def in_hbm(x):
    return pltpu.with_memory_space_constraint(x, pltpu.HBM)


def in_vmem():
    return pl.BlockSpec(memory_space=pltpu.VMEM)


def run_mixer(
    u, sr, si, decay, freq, log_step, inr, ini, cr, ci, skip, gv, gg, res, mix, gain, routes
):
    seq, width = u.shape
    model = res.shape[1]
    steps = 4
    groups, states = decay.shape
    part = model // PARTS
    gb, cb, wb = groups // steps, width // steps, groups * states // steps
    cols = lambda n: pl.BlockSpec((seq, n), lambda i: (0, i))
    rows = lambda r, n: pl.BlockSpec((r, n), lambda i: (i, 0))
    whole = lambda x: pl.BlockSpec(x.shape, lambda i: (0, 0))
    out_rows = 128 * CAPACITY * PARTS
    return pl.pallas_call(
        mixer_kernel,
        grid=(steps,),
        in_specs=[
            cols(cb), cols(wb), cols(wb), rows(gb, states), rows(gb, states), whole(log_step),
            rows(cb, states), rows(cb, states), rows(cb, states), rows(cb, states),
            pl.BlockSpec((1, cb), lambda i: (0, i)),
            rows(cb, model), rows(cb, model), whole(res), whole(mix), whole(gain), whole(routes),
        ],
        out_specs=[
            cols(wb), cols(wb),
            in_vmem(), in_vmem(), in_vmem(),
        ],
        out_shape=[
            jax.ShapeDtypeStruct(sr.shape, f32),
            jax.ShapeDtypeStruct(si.shape, f32),
            jax.ShapeDtypeStruct((seq, model), bf16),
            jax.ShapeDtypeStruct((seq, model), bf16),
            jax.ShapeDtypeStruct((out_rows, part), bf16),
        ],
        scratch_shapes=[pltpu.VMEM((cb, wb), bf16)] * 4 + [pltpu.VMEM((seq, model), f32)] * 2,
        compiler_params=pltpu.CompilerParams(vmem_limit_bytes=24 << 20),
        name="mixer",
    )(*map(
        in_hbm,
        (u, sr, si, decay, freq, log_step, inr, ini, cr, ci, skip, gv, gg, res, mix, gain, routes),
    ))


def swap_matrix(back):
    i = iota((CHUNK, CHUNK), 1 if back else 0)
    j = iota((CHUNK, CHUNK), 0 if back else 1)
    source = ((i // 4) % 16) * 16 + (i // 64) * 4 + i % 4
    return jnp.where(source == j, 1.0, 0.0).astype(bf16)


def expert_kernel(y_ref, wg_ref, wu_ref, wd_ref, z_ref, x_ref, h_ref, held, sems):
    model = wg_ref.shape[0]
    part = model // PARTS
    take = CHUNK // PARTS
    order = swap_matrix(False)
    chunks = y_ref.shape[0] // CHUNK
    for c in range(chunks):
        x = dot(order, y_ref[CHUNK * c : CHUNK * (c + 1), :]).astype(bf16)
        for q in range(PARTS):
            x_ref[take * c : take * (c + 1), part * q : part * (q + 1)] = x[take * q : take * (q + 1)]
    gate = dot(x_ref[...], wg_ref[...])
    up = dot(x_ref[...], wu_ref[...])
    h_ref[...] = (gate * jax.nn.sigmoid(gate) * up).astype(bf16)
    back = swap_matrix(True)
    halves = sems.shape[0]
    rows = h_ref.shape[0] // halves
    copies = []
    for h in range(halves):
        out = dot(h_ref[rows * h : rows * (h + 1), :], wd_ref[...]).astype(bf16)
        for c in range(rows // take):
            o = out[take * c : take * (c + 1)]
            o = jnp.concatenate([o[:, part * q : part * (q + 1)] for q in range(PARTS)], axis=0)
            first = PARTS * rows * h + CHUNK * c
            held[first : first + CHUNK, :] = dot(back, o).astype(bf16)
        span = pl.ds(PARTS * rows * h, PARTS * rows)
        copy = pltpu.make_async_copy(held.at[span], z_ref.at[span], sems.at[h])
        copy.start()
        copies.append(copy)
    for copy in copies:
        copy.wait()


def run_expert(y, wg, wu, wd):
    rows = y.shape[0] // PARTS
    return pl.pallas_call(
        expert_kernel,
        in_specs=[in_vmem()] * 4,
        out_specs=pl.BlockSpec(memory_space=pltpu.HBM),
        out_shape=pltpu.HBM(y.shape, bf16),
        scratch_shapes=[
            pltpu.VMEM((rows, wg.shape[0]), bf16),
            pltpu.VMEM((rows, wg.shape[1]), bf16),
            pltpu.VMEM(y.shape, bf16),
            pltpu.SemaphoreType.DMA((2,)),
        ],
        compiler_params=pltpu.CompilerParams(vmem_limit_bytes=20 << 20),
        name="expert",
    )(y, wg, wu, wd)


def shared_kernel(normed_ref, wg_ref, wu_ref, wd_ref, routes_ref, weights_ref, out_ref, mix_ref):
    x = normed_ref[...]
    gate = dot(x, wg_ref[...])
    up = dot(x, wu_ref[...])
    hidden = (gate * jax.nn.sigmoid(gate) * up).astype(bf16)
    out_ref[...] = dot(hidden, wd_ref[...])

    routes = routes_ref[...]
    weights = weights_ref[...]
    top, seq = routes.shape
    code = route_code(routes)
    row = iota(code.shape, 0)
    weight = jnp.zeros(code.shape, f32)
    for k in range(top):
        weight = weight + jnp.where(row == routes[k : k + 1, :], weights[k : k + 1, :], 0.0)
    code = jnp.concatenate([code] * PARTS, axis=1)
    weight = jnp.concatenate([weight] * PARTS, axis=1)
    hi, lo = split(weight)
    want = slot_pattern(seq)
    for c in range(mix_ref.shape[1] // CHUNK):
        r = slice(16 * c, 16 * (c + 1))
        hit = spread_rows(code[r]) == want
        for h, w in enumerate((hi, lo)):
            mix_ref[PARTS * seq * h : PARTS * seq * (h + 1), CHUNK * c : CHUNK * (c + 1)] = (
                jnp.where(hit, spread_rows(w[r]), 0.0).T.astype(bf16)
            )


def run_shared(normed, wg, wu, wd, routes, weights):
    seq, model = normed.shape
    return pl.pallas_call(
        shared_kernel,
        out_shape=[
            jax.ShapeDtypeStruct((seq, model), f32),
            pltpu.VMEM((2 * PARTS * seq, 128 * CAPACITY * PARTS), bf16),
        ],
        in_specs=[in_vmem()] * 6,
        out_specs=[in_vmem()] * 2,
        compiler_params=pltpu.CompilerParams(vmem_limit_bytes=16 << 20),
        cost_estimate=pl.CostEstimate(
            flops=2 * seq * model * wg.shape[1] * 60, bytes_accessed=8 << 20, transcendentals=0
        ),
        name="shared",
    )(normed, wg, wu, wd, routes, weights)


def combine_kernel(z_ref, mix_ref, shared_ref, mid_ref, gain_ref, out_ref):
    seq = mid_ref.shape[0]
    both = dot(mix_ref[...], z_ref[...])
    both = both[: PARTS * seq] + both[PARTS * seq :]
    routed = jnp.concatenate([both[seq * q : seq * (q + 1)] for q in range(PARTS)], axis=1)
    combined = shared_ref[...] + routed
    out_ref[...] = (
        mid_ref[...].astype(f32) + combined * rms_scale(combined) * gain_ref[...]
    ).astype(bf16)


def run_combine(z, mix, shared, mid, gain):
    return pl.pallas_call(
        combine_kernel,
        out_shape=jax.ShapeDtypeStruct(mid.shape, bf16),
        in_specs=[in_vmem()] * 5,
        out_specs=in_vmem(),
        compiler_params=pltpu.CompilerParams(vmem_limit_bytes=16 << 20),
        name="combine",
    )(z, mix, shared, mid, gain)


def per_device(
    residual, branch_in, state_real, state_imag, decay_rate, frequency, log_step, input_real,
    input_imag, output_matrix_real, output_matrix_imaginary, skip_gain, glu_value, glu_gate,
    mix_gain, moe_in_gain, moe_out_gain, routes, route_weights, expert_gate, expert_up,
    expert_down, shared_gate, shared_up, shared_down,
):
    states = decay_rate.shape[1]
    model = residual.shape[1]
    part = model // PARTS
    row = lambda v: v.reshape(1, -1)
    inr = jnp.transpose(input_real, (0, 2, 1)).reshape(-1, states)
    ini = jnp.transpose(input_imag, (0, 2, 1)).reshape(-1, states)
    cr = output_matrix_real.reshape(-1, states)
    ci = output_matrix_imaginary.reshape(-1, states)
    routes_t = routes.T
    weights_t = route_weights.T
    next_real, next_imag, mid, normed, outgoing = run_mixer(
        branch_in, state_real, state_imag, decay_rate, frequency, row(log_step), inr, ini, cr, ci,
        row(skip_gain), glu_value, glu_gate, residual, row(mix_gain), row(moe_in_gain), routes_t,
    )

    def exchange(x):
        x = x.reshape(128, PARTS * CAPACITY, part)
        return lax.all_to_all(x, "ep", split_axis=0, concat_axis=0, tiled=True).reshape(-1, part)

    arrived = exchange(outgoing)
    shared, mix = run_shared(normed, shared_gate, shared_up, shared_down, routes_t, weights_t)
    returned = exchange(run_expert(arrived, expert_gate[0], expert_up[0], expert_down[0]))
    layer_out = run_combine(returned, mix, shared, mid, row(moe_out_gain))
    return layer_out, next_real, next_imag


def solution(mesh):
    rows2 = P("ep", None)
    rows3 = P("ep", None, None)
    return jax.shard_map(
        per_device,
        mesh=mesh,
        in_specs=(rows2,) * 4 + (P(),) * 13 + (rows2,) * 2 + (rows3,) * 3 + (P(),) * 3,
        out_specs=(rows2, rows2, rows2),
        check_vma=False,
    )
```

```python
import functools

import jax
import jax.numpy as jnp
from jax import lax
from jax.experimental import pallas as pl
from jax.experimental.pallas import tpu as pltpu
from jax.sharding import PartitionSpec as P

norm_eps = 1e-06
f32 = jnp.float32
bf16 = jnp.bfloat16

CHUNK = 256
CAPACITY = 4
PARTS = 4


def iota(shape, dim):
    return lax.broadcasted_iota(jnp.int32, shape, dim)


def dot(a, b):
    return jnp.dot(a, b, preferred_element_type=f32)


def sin_cos(x):
    turns = jnp.floor(x * 0.6366197723675814 + 0.5)
    r = ((x - turns * 1.5703125) - turns * 4.837512969970703125e-4) - turns * 7.54978995489188216e-8
    z = r * r
    s = r + r * z * ((-1.9515295891e-4 * z + 8.3321608736e-3) * z - 1.6666654611e-1)
    c = 1.0 - 0.5 * z + z * z * (
        (2.443315711809948e-5 * z - 1.388731625493765e-3) * z + 4.166664568298827e-2
    )
    quarter = turns.astype(jnp.int32) & 3
    odd = (quarter & 1) == 1
    sin_x = jnp.where(odd, c, s)
    cos_x = jnp.where(odd, s, c)
    sin_x = jnp.where(quarter >= 2, -sin_x, sin_x)
    cos_x = jnp.where((quarter == 1) | (quarter == 2), -cos_x, cos_x)
    return sin_x, cos_x


def split(x):
    hi = x.astype(bf16)
    return hi, (x - hi.astype(f32)).astype(bf16)


def route_code(routes):
    top, seq = routes.shape
    experts = 128
    row = iota((experts, seq), 0)
    named = jnp.zeros((experts, seq), f32)
    for k in range(top):
        named = named + jnp.where(row == routes[k : k + 1, :], 1.0, 0.0)
    before = jnp.where(iota((seq, seq), 0) < iota((seq, seq), 1), 1.0, 0.0).astype(bf16)
    rank = dot(named.astype(bf16), before)
    return jnp.where(named > 0.5, rank, -1.0)


def spread_rows(block):
    one_hot = jnp.where(iota((CHUNK, 16), 0) // 16 == iota((CHUNK, 16), 1), 1.0, 0.0)
    return dot(one_hot.astype(bf16), block.astype(bf16))


def slot_pattern(seq):
    i = iota((CHUNK, PARTS * seq), 0)
    j = iota((CHUNK, PARTS * seq), 1)
    return jnp.where((i // 4) % 4 == j // seq, (i % 4).astype(f32), -2.0)


def rms_scale(x):
    return lax.rsqrt(jnp.mean(x * x, axis=-1, keepdims=True) + norm_eps)


MIXER_INS = 17


def mixer_kernel(*refs):
    hbm = refs[:MIXER_INS]
    nr_ref, ni_ref, mid_ref, normed_ref, out_ref = refs[MIXER_INS : MIXER_INS + 5]
    local = refs[MIXER_INS + 5 : 2 * MIXER_INS + 5]
    nr, ni, select, small_sems, state_sems, glu_sems, out_sems = refs[2 * MIXER_INS + 5 :]
    (u_v, sr, si, decay_v, freq_v, log_v, inr, ini, cr, ci,
     skip_v, gv, gg, res_v, mix_v, gain_v, routes_v) = local

    def copies_of(index, count, axis, sems, first):
        size = hbm[index].shape[axis] // count
        made = []
        for k in range(count):
            span = pl.ds(size * k, size)
            at = (slice(None), span) if axis else (span, slice(None))
            made.append(
                pltpu.make_async_copy(hbm[index].at[at], local[index].at[at], sems.at[first + k])
            )
        return made

    cuts = 4
    small = {}
    for n, index in enumerate((3, 4, 5, 16, 0, 6, 7, 8, 9, 10, 13, 14, 15)):
        small[index] = copies_of(index, 1, 0, small_sems, n)[0]
    state = [copies_of(1, cuts, 1, state_sems, 0), copies_of(2, cuts, 1, state_sems, cuts)]
    value = copies_of(11, cuts, 0, glu_sems, 0)
    gate = copies_of(12, cuts, 0, glu_sems, cuts)
    for index in (3, 4, 5, 16, 0, 6, 7):
        small[index].start()
    for j in range(cuts):
        state[0][j].start()
        state[1][j].start()
        if j == 0:
            for index in (8, 9, 10):
                small[index].start()
    for copy in value:
        copy.start()
    for index in (13, 14, 15):
        small[index].start()
    for copy in gate:
        copy.start()

    seq = u_v.shape[0]
    groups, states = decay_v.shape
    packed = 4
    wide = packed * states
    cols = u_v.shape[1] // cuts
    chans = cols // (groups // cuts)

    small[16].wait()
    code = route_code(routes_v[...])
    code = jnp.concatenate([code] * PARTS, axis=1)
    want = slot_pattern(seq)
    for c in range(select.shape[0] // CHUNK):
        here = spread_rows(code[16 * c : 16 * (c + 1)])
        select[CHUNK * c : CHUNK * (c + 1), :] = jnp.where(here == want, 1.0, 0.0).astype(bf16)

    small[5].wait()
    small[3].wait()
    small[4].wait()
    pick = iota((groups, groups), 1) == iota((groups, groups), 0)
    step_size = jnp.exp(jnp.sum(jnp.where(pick, log_v[...], 0.0), axis=1, keepdims=True))
    decay = decay_v[...]
    freq = freq_v[...]
    magnitude = jnp.exp(-decay * step_size)
    sin_x, cos_x = sin_cos(freq * step_size)
    a_re = magnitude * cos_x
    a_im = magnitude * sin_x
    lam = -decay
    den = lam * lam + freq * freq
    num = a_re - 1.0
    k_re = (num * lam + a_im * freq) / den
    k_im = (a_im * lam - num * freq) / den
    own = iota((groups, wide), 0) % packed == iota((groups, wide), 1) // states

    def tiled(x):
        twice = jnp.concatenate([x, x], axis=1)
        return jnp.concatenate([twice] * (packed // 2), axis=1)

    def flat(x):
        x = jnp.where(own, tiled(x), 0.0)
        return [
            jnp.sum(x[packed * b : packed * (b + 1)], axis=0, keepdims=True)
            for b in range(groups // packed)
        ]

    a_re, a_im, k_re, k_im = flat(a_re), flat(a_im), flat(k_re), flat(k_im)

    patch = (iota((cols, wide), 0) // chans) % packed == iota((cols, wide), 1) // states

    def weights(ref, j):
        x = ref[cols * j : cols * (j + 1), :].astype(f32)
        return jnp.where(patch, tiled(x), 0.0).astype(bf16)

    lane = iota((seq, cols), 1) // (cols // packed)
    for index in (0, 6, 7):
        small[index].wait()
    outs = []
    acts = []
    for j in range(cuts):
        u = u_v[:, cols * j : cols * (j + 1)].astype(f32)
        spread = jnp.concatenate(
            [jnp.where(lane == k, u, 0.0) for k in range(packed)], axis=0
        ).astype(bf16)
        f_re = dot(spread, weights(inr, j))
        f_im = dot(spread, weights(ini, j))
        state[0][j].wait()
        state[1][j].wait()
        fresh_re, fresh_im = [], []
        for k in range(packed):
            b = packed * j + k
            at = slice(wide * b, wide * (b + 1))
            r = slice(seq * k, seq * (k + 1))
            old_re = sr[:, at]
            old_im = si[:, at]
            new_re = a_re[b] * old_re - a_im[b] * old_im + (k_re[b] * f_re[r] - k_im[b] * f_im[r])
            new_im = a_re[b] * old_im + a_im[b] * old_re + (k_re[b] * f_im[r] + k_im[b] * f_re[r])
            nr[:, at] = new_re
            ni[:, at] = new_im
            fresh_re.append(new_re)
            fresh_im.append(new_im)
        for n, (src, dst) in enumerate(((nr, nr_ref), (ni, ni_ref))):
            at = (slice(None), pl.ds(packed * wide * j, packed * wide))
            copy = pltpu.make_async_copy(src.at[at], dst.at[at], out_sems.at[cuts * n + j])
            copy.start()
            outs.append(copy)
        if j == 0:
            for index in (8, 9, 10):
                small[index].wait()

        def read(parts, ref):
            pairs = [split(x) for x in parts]
            rows = jnp.concatenate([p[0] for p in pairs] + [p[1] for p in pairs], axis=0)
            got = lax.dot_general(
                rows, weights(ref, j), (((1,), (1,)), ((), ())), preferred_element_type=f32
            )
            return got[: packed * seq] + got[packed * seq :]

        both = read(fresh_re, cr) - read(fresh_im, ci)
        readout = both[:seq]
        for k in range(1, packed):
            readout = jnp.where(lane == k, both[seq * k : seq * (k + 1)], readout)
        mixed = readout + skip_v[:, cols * j : cols * (j + 1)] * u
        acts.append(jax.nn.gelu(mixed).astype(bf16))

    act = jnp.concatenate(acts, axis=1)
    for copy in value:
        copy.wait()
    value_part = dot(act, gv[...])
    for copy in gate:
        copy.wait()
    branch = value_part * jax.nn.sigmoid(dot(act, gg[...]))
    for index in (13, 14, 15):
        small[index].wait()
    mid = (res_v[...].astype(f32) + branch * rms_scale(branch) * mix_v[...]).astype(bf16)
    mid_ref[...] = mid
    mid = mid.astype(f32)
    normed = (mid * rms_scale(mid) * gain_v[...]).astype(bf16)
    normed_ref[...] = normed
    part = normed.shape[1] // PARTS
    stacked = jnp.concatenate(
        [normed[:, part * q : part * (q + 1)] for q in range(PARTS)], axis=0
    )
    out_ref[...] = dot(select[...], stacked).astype(bf16)
    for copy in outs:
        copy.wait()


def in_hbm(x):
    return pltpu.with_memory_space_constraint(x, pltpu.HBM)


def in_vmem():
    return pl.BlockSpec(memory_space=pltpu.VMEM)


def run_mixer(*operands):
    seq, model = operands[13].shape
    state = operands[1].shape
    part = model // PARTS
    out_rows = 128 * CAPACITY * PARTS
    return pl.pallas_call(
        mixer_kernel,
        in_specs=[pl.BlockSpec(memory_space=pltpu.HBM)] * MIXER_INS,
        out_specs=[pl.BlockSpec(memory_space=pltpu.HBM)] * 2 + [in_vmem()] * 3,
        out_shape=[
            pltpu.HBM(state, f32),
            pltpu.HBM(state, f32),
            jax.ShapeDtypeStruct((seq, model), bf16),
            jax.ShapeDtypeStruct((seq, model), bf16),
            jax.ShapeDtypeStruct((out_rows, part), bf16),
        ],
        scratch_shapes=[pltpu.VMEM(x.shape, x.dtype) for x in operands]
        + [
            pltpu.VMEM(state, f32),
            pltpu.VMEM(state, f32),
            pltpu.VMEM((out_rows, PARTS * seq), bf16),
            pltpu.SemaphoreType.DMA((13,)),
            pltpu.SemaphoreType.DMA((8,)),
            pltpu.SemaphoreType.DMA((8,)),
            pltpu.SemaphoreType.DMA((8,)),
        ],
        compiler_params=pltpu.CompilerParams(vmem_limit_bytes=28 << 20),
        name="mixer",
    )(*map(in_hbm, operands))


def swap_matrix(back):
    i = iota((CHUNK, CHUNK), 1 if back else 0)
    j = iota((CHUNK, CHUNK), 0 if back else 1)
    source = ((i // 4) % 16) * 16 + (i // 64) * 4 + i % 4
    return jnp.where(source == j, 1.0, 0.0).astype(bf16)


def expert_kernel(y_ref, wg_ref, wu_ref, wd_ref, z_ref, x_ref, h_ref, held, sems):
    model = wg_ref.shape[0]
    part = model // PARTS
    take = CHUNK // PARTS
    order = swap_matrix(False)
    chunks = y_ref.shape[0] // CHUNK
    for c in range(chunks):
        x = dot(order, y_ref[CHUNK * c : CHUNK * (c + 1), :]).astype(bf16)
        for q in range(PARTS):
            x_ref[take * c : take * (c + 1), part * q : part * (q + 1)] = x[take * q : take * (q + 1)]
    gate = dot(x_ref[...], wg_ref[...])
    up = dot(x_ref[...], wu_ref[...])
    h_ref[...] = (gate * jax.nn.sigmoid(gate) * up).astype(bf16)
    back = swap_matrix(True)
    halves = sems.shape[0]
    rows = h_ref.shape[0] // halves
    copies = []
    for h in range(halves):
        out = dot(h_ref[rows * h : rows * (h + 1), :], wd_ref[...]).astype(bf16)
        for c in range(rows // take):
            o = out[take * c : take * (c + 1)]
            o = jnp.concatenate([o[:, part * q : part * (q + 1)] for q in range(PARTS)], axis=0)
            first = PARTS * rows * h + CHUNK * c
            held[first : first + CHUNK, :] = dot(back, o).astype(bf16)
        span = pl.ds(PARTS * rows * h, PARTS * rows)
        copy = pltpu.make_async_copy(held.at[span], z_ref.at[span], sems.at[h])
        copy.start()
        copies.append(copy)
    for copy in copies:
        copy.wait()


def run_expert(y, wg, wu, wd):
    rows = y.shape[0] // PARTS
    return pl.pallas_call(
        expert_kernel,
        in_specs=[in_vmem()] * 4,
        out_specs=pl.BlockSpec(memory_space=pltpu.HBM),
        out_shape=pltpu.HBM(y.shape, bf16),
        scratch_shapes=[
            pltpu.VMEM((rows, wg.shape[0]), bf16),
            pltpu.VMEM((rows, wg.shape[1]), bf16),
            pltpu.VMEM(y.shape, bf16),
            pltpu.SemaphoreType.DMA((2,)),
        ],
        compiler_params=pltpu.CompilerParams(vmem_limit_bytes=20 << 20),
        name="expert",
    )(y, wg, wu, wd)


def shared_kernel(normed_ref, wg_ref, wu_ref, wd_ref, routes_ref, weights_ref, out_ref, mix_ref):
    x = normed_ref[...]
    gate = dot(x, wg_ref[...])
    up = dot(x, wu_ref[...])
    hidden = (gate * jax.nn.sigmoid(gate) * up).astype(bf16)
    out_ref[...] = dot(hidden, wd_ref[...])

    routes = routes_ref[...]
    weights = weights_ref[...]
    top, seq = routes.shape
    code = route_code(routes)
    row = iota(code.shape, 0)
    weight = jnp.zeros(code.shape, f32)
    for k in range(top):
        weight = weight + jnp.where(row == routes[k : k + 1, :], weights[k : k + 1, :], 0.0)
    code = jnp.concatenate([code, code], axis=1)
    weight = jnp.concatenate(split(weight), axis=1)
    slot = (iota((CHUNK, 2 * seq), 0) % CAPACITY).astype(f32)
    for c in range(mix_ref.shape[1] // CHUNK):
        r = slice(16 * c, 16 * (c + 1))
        hit = spread_rows(code[r]) == slot
        mix_ref[:, CHUNK * c : CHUNK * (c + 1)] = (
            jnp.where(hit, spread_rows(weight[r]), 0.0).T.astype(bf16)
        )


def run_shared(normed, wg, wu, wd, routes, weights):
    seq, model = normed.shape
    return pl.pallas_call(
        shared_kernel,
        out_shape=[
            jax.ShapeDtypeStruct((seq, model), f32),
            jax.ShapeDtypeStruct((2 * seq, 128 * CAPACITY * PARTS), bf16),
        ],
        in_specs=[in_vmem()] * 6,
        out_specs=[in_vmem()] * 2,
        compiler_params=pltpu.CompilerParams(vmem_limit_bytes=16 << 20),
        cost_estimate=pl.CostEstimate(
            flops=2 * seq * model * wg.shape[1] * 60, bytes_accessed=8 << 20, transcendentals=0
        ),
        name="shared",
    )(normed, wg, wu, wd, routes, weights)


def combine_kernel(z_ref, mix_ref, shared_ref, mid_ref, gain_ref, out_ref):
    seq = mid_ref.shape[0]
    mix = mix_ref[...]
    part_of = (iota((1, mix.shape[1]), 1) // CAPACITY) % PARTS
    rows = [mix * jnp.where(part_of == q, 1.0, 0.0).astype(bf16) for q in range(PARTS)]
    both = dot(jnp.concatenate(rows, axis=0), z_ref[...])
    routed = jnp.concatenate(
        [
            both[2 * seq * q : 2 * seq * q + seq] + both[2 * seq * q + seq : 2 * seq * (q + 1)]
            for q in range(PARTS)
        ],
        axis=1,
    )
    combined = shared_ref[...] + routed
    out_ref[...] = (
        mid_ref[...].astype(f32) + combined * rms_scale(combined) * gain_ref[...]
    ).astype(bf16)


def run_combine(z, mix, shared, mid, gain):
    return pl.pallas_call(
        combine_kernel,
        out_shape=jax.ShapeDtypeStruct(mid.shape, bf16),
        in_specs=[in_vmem()] * 5,
        out_specs=in_vmem(),
        compiler_params=pltpu.CompilerParams(vmem_limit_bytes=16 << 20),
        name="combine",
    )(z, mix, shared, mid, gain)


def per_device(
    residual, branch_in, state_real, state_imag, decay_rate, frequency, log_step, input_real,
    input_imag, output_matrix_real, output_matrix_imaginary, skip_gain, glu_value, glu_gate,
    mix_gain, moe_in_gain, moe_out_gain, routes, route_weights, expert_gate, expert_up,
    expert_down, shared_gate, shared_up, shared_down,
):
    states = decay_rate.shape[1]
    model = residual.shape[1]
    part = model // PARTS
    row = lambda v: v.reshape(1, -1)
    inr = jnp.transpose(input_real, (0, 2, 1)).reshape(-1, states)
    ini = jnp.transpose(input_imag, (0, 2, 1)).reshape(-1, states)
    cr = output_matrix_real.reshape(-1, states)
    ci = output_matrix_imaginary.reshape(-1, states)
    routes_t = routes.T
    weights_t = route_weights.T
    next_real, next_imag, mid, normed, outgoing = run_mixer(
        branch_in, state_real, state_imag, decay_rate, frequency, row(log_step), inr, ini, cr, ci,
        row(skip_gain), glu_value, glu_gate, residual, row(mix_gain), row(moe_in_gain), routes_t,
    )

    def exchange(x):
        x = x.reshape(128, PARTS * CAPACITY, part)
        return lax.all_to_all(x, "ep", split_axis=0, concat_axis=0, tiled=True).reshape(-1, part)

    arrived = exchange(outgoing)
    shared, mix = run_shared(normed, shared_gate, shared_up, shared_down, routes_t, weights_t)
    returned = exchange(run_expert(arrived, expert_gate[0], expert_up[0], expert_down[0]))
    layer_out = run_combine(returned, mix, shared, mid, row(moe_out_gain))
    return layer_out, next_real, next_imag


def solution(mesh):
    rows2 = P("ep", None)
    rows3 = P("ep", None, None)
    return jax.shard_map(
        per_device,
        mesh=mesh,
        in_specs=(rows2,) * 4 + (P(),) * 13 + (rows2,) * 2 + (rows3,) * 3 + (P(),) * 3,
        out_specs=(rows2, rows2, rows2),
        check_vma=False,
    )
```

```python
import functools

import jax
import jax.numpy as jnp
from jax import lax
from jax.experimental import pallas as pl
from jax.experimental.pallas import tpu as pltpu
from jax.sharding import PartitionSpec as P

norm_eps = 1e-06
f32 = jnp.float32
bf16 = jnp.bfloat16

CHUNK = 256
CAPACITY = 4
PARTS = 4


def iota(shape, dim):
    return lax.broadcasted_iota(jnp.int32, shape, dim)


def dot(a, b):
    return jnp.dot(a, b, preferred_element_type=f32)


def sin_cos(x):
    turns = jnp.floor(x * 0.6366197723675814 + 0.5)
    r = ((x - turns * 1.5703125) - turns * 4.837512969970703125e-4) - turns * 7.54978995489188216e-8
    z = r * r
    s = r + r * z * ((-1.9515295891e-4 * z + 8.3321608736e-3) * z - 1.6666654611e-1)
    c = 1.0 - 0.5 * z + z * z * (
        (2.443315711809948e-5 * z - 1.388731625493765e-3) * z + 4.166664568298827e-2
    )
    quarter = turns.astype(jnp.int32) & 3
    odd = (quarter & 1) == 1
    sin_x = jnp.where(odd, c, s)
    cos_x = jnp.where(odd, s, c)
    sin_x = jnp.where(quarter >= 2, -sin_x, sin_x)
    cos_x = jnp.where((quarter == 1) | (quarter == 2), -cos_x, cos_x)
    return sin_x, cos_x


def route_code(routes):
    top, seq = routes.shape
    experts = 128
    row = iota((experts, seq), 0)
    named = jnp.zeros((experts, seq), f32)
    for k in range(top):
        named = named + jnp.where(row == routes[k : k + 1, :], 1.0, 0.0)
    before = jnp.where(iota((seq, seq), 0) < iota((seq, seq), 1), 1.0, 0.0).astype(bf16)
    rank = dot(named.astype(bf16), before)
    return jnp.where(named > 0.5, rank, -1.0)


def spread_rows(block):
    one_hot = jnp.where(iota((CHUNK, 16), 0) // 16 == iota((CHUNK, 16), 1), 1.0, 0.0)
    return dot(one_hot.astype(bf16), block.astype(bf16))


def slot_pattern(seq):
    i = iota((CHUNK, PARTS * seq), 0)
    j = iota((CHUNK, PARTS * seq), 1)
    return jnp.where((i // 4) % 4 == j // seq, (i % 4).astype(f32), -2.0)


def rms_scale(x):
    return lax.rsqrt(jnp.mean(x * x, axis=-1, keepdims=True) + norm_eps)


MIXER_INS = 17


def mixer_kernel(*refs):
    hbm = refs[:MIXER_INS]
    nr_ref, ni_ref, mid_ref, normed_ref, out_ref = refs[MIXER_INS : MIXER_INS + 5]
    local = refs[MIXER_INS + 5 : 2 * MIXER_INS + 5]
    nr, ni, select, force_re, force_im, read_re, read_im, small_sems, state_sems, glu_sems, out_sems = refs[2 * MIXER_INS + 5 :]
    (u_v, sr, si, decay_v, freq_v, log_v, inr, ini, cr, ci,
     skip_v, gv, gg, res_v, mix_v, gain_v, routes_v) = local

    def copies_of(index, count, axis, sems, first):
        size = hbm[index].shape[axis] // count
        made = []
        for k in range(count):
            span = pl.ds(size * k, size)
            at = (slice(None), span) if axis else (span, slice(None))
            made.append(
                pltpu.make_async_copy(hbm[index].at[at], local[index].at[at], sems.at[first + k])
            )
        return made

    cuts = 4
    small = {}
    for n, index in enumerate((3, 4, 5, 16, 0, 6, 7, 8, 9, 10, 13, 14, 15)):
        small[index] = copies_of(index, 1, 0, small_sems, n)[0]
    state = [copies_of(1, cuts, 1, state_sems, 0), copies_of(2, cuts, 1, state_sems, cuts)]
    glu_cuts = glu_sems.shape[0] // 2
    value = copies_of(11, glu_cuts, 1, glu_sems, 0)
    gate = copies_of(12, glu_cuts, 1, glu_sems, glu_cuts)
    for index in (3, 4, 5, 16, 0, 6, 7, 8, 9, 10):
        small[index].start()
    for j in range(cuts):
        state[0][j].start()
        state[1][j].start()
    for n in range(glu_cuts):
        value[n].start()
        gate[n].start()
    for index in (13, 14, 15):
        small[index].start()

    seq = u_v.shape[0]
    groups, states = decay_v.shape
    packed = 4
    wide = packed * states
    cols = u_v.shape[1] // cuts
    chans = cols // (groups // cuts)

    small[16].wait()
    code = route_code(routes_v[...])
    code = jnp.concatenate([code] * PARTS, axis=1)
    want = slot_pattern(seq)
    for c in range(select.shape[0] // CHUNK):
        here = spread_rows(code[16 * c : 16 * (c + 1)])
        select[CHUNK * c : CHUNK * (c + 1), :] = jnp.where(here == want, 1.0, 0.0).astype(bf16)

    small[5].wait()
    small[3].wait()
    small[4].wait()
    pick = iota((groups, groups), 1) == iota((groups, groups), 0)
    step_size = jnp.exp(jnp.sum(jnp.where(pick, log_v[...], 0.0), axis=1, keepdims=True))
    decay = decay_v[...]
    freq = freq_v[...]
    magnitude = jnp.exp(-decay * step_size)
    sin_x, cos_x = sin_cos(freq * step_size)
    a_re = magnitude * cos_x
    a_im = magnitude * sin_x
    lam = -decay
    den = lam * lam + freq * freq
    num = a_re - 1.0
    k_re = (num * lam + a_im * freq) / den
    k_im = (a_im * lam - num * freq) / den
    own = iota((groups, wide), 0) % packed == iota((groups, wide), 1) // states

    def tiled(x):
        twice = jnp.concatenate([x, x], axis=1)
        return jnp.concatenate([twice] * (packed // 2), axis=1)

    def flat(x):
        x = jnp.where(own, tiled(x), 0.0)
        return [
            jnp.sum(x[packed * b : packed * (b + 1)], axis=0, keepdims=True)
            for b in range(groups // packed)
        ]

    a_re, a_im, k_re, k_im = flat(a_re), flat(a_im), flat(k_re), flat(k_im)

    patch = (iota((cols, wide), 0) // chans) % packed == iota((cols, wide), 1) // states

    def weights(ref, j):
        x = ref[cols * j : cols * (j + 1), :].astype(f32)
        return jnp.where(patch, tiled(x), 0.0).astype(bf16)

    lane = iota((seq, cols), 1) // (cols // packed)
    for index in (0, 6, 7):
        small[index].wait()
    for j in range(cuts):
        u = u_v[:, cols * j : cols * (j + 1)].astype(f32)
        spread = jnp.concatenate(
            [jnp.where(lane == k, u, 0.0) for k in range(packed)], axis=0
        ).astype(bf16)
        force_re[j] = dot(spread, weights(inr, j))
        force_im[j] = dot(spread, weights(ini, j))
    for index in (8, 9, 10):
        small[index].wait()
    for j in range(cuts):
        read_re[j] = weights(cr, j)
        read_im[j] = weights(ci, j)

    outs = []
    acts = []
    for j in range(cuts):
        u = u_v[:, cols * j : cols * (j + 1)].astype(f32)
        f_re = force_re[j]
        f_im = force_im[j]
        state[0][j].wait()
        state[1][j].wait()
        fresh_re, fresh_im = [], []
        for k in range(packed):
            b = packed * j + k
            at = slice(wide * b, wide * (b + 1))
            r = slice(seq * k, seq * (k + 1))
            old_re = sr[:, at]
            old_im = si[:, at]
            new_re = a_re[b] * old_re - a_im[b] * old_im + (k_re[b] * f_re[r] - k_im[b] * f_im[r])
            new_im = a_re[b] * old_im + a_im[b] * old_re + (k_re[b] * f_im[r] + k_im[b] * f_re[r])
            nr[:, at] = new_re
            ni[:, at] = new_im
            fresh_re.append(new_re)
            fresh_im.append(new_im)
        for n, (src, dst) in enumerate(((nr, nr_ref), (ni, ni_ref))):
            at = (slice(None), pl.ds(packed * wide * j, packed * wide))
            copy = pltpu.make_async_copy(src.at[at], dst.at[at], out_sems.at[cuts * n + j])
            outs.append(copy)

        def read(parts, ref):
            rows = jnp.concatenate([x.astype(bf16) for x in parts], axis=0)
            return lax.dot_general(
                rows, ref[j], (((1,), (1,)), ((), ())), preferred_element_type=f32
            )

        both = read(fresh_re, read_re) - read(fresh_im, read_im)
        readout = both[:seq]
        for k in range(1, packed):
            readout = jnp.where(lane == k, both[seq * k : seq * (k + 1)], readout)
        mixed = readout + skip_v[:, cols * j : cols * (j + 1)] * u
        acts.append(jax.nn.gelu(mixed).astype(bf16))

    act = jnp.concatenate(acts, axis=1)
    piece = gv.shape[1] // glu_cuts
    pieces = []
    for n in range(glu_cuts):
        at = slice(piece * n, piece * (n + 1))
        value[n].wait()
        value_part = dot(act, gv[:, at])
        gate[n].wait()
        if n == glu_cuts - 1:
            for copy in outs:
                copy.start()
        pieces.append(value_part * jax.nn.sigmoid(dot(act, gg[:, at])))
    branch = jnp.concatenate(pieces, axis=1)
    for index in (13, 14, 15):
        small[index].wait()
    mid = (res_v[...].astype(f32) + branch * rms_scale(branch) * mix_v[...]).astype(bf16)
    mid_ref[...] = mid
    mid = mid.astype(f32)
    normed = (mid * rms_scale(mid) * gain_v[...]).astype(bf16)
    normed_ref[...] = normed
    part = normed.shape[1] // PARTS
    stacked = jnp.concatenate(
        [normed[:, part * q : part * (q + 1)] for q in range(PARTS)], axis=0
    )
    out_ref[...] = dot(select[...], stacked).astype(bf16)
    for copy in outs:
        copy.wait()


def in_hbm(x):
    return pltpu.with_memory_space_constraint(x, pltpu.HBM)


def in_vmem():
    return pl.BlockSpec(memory_space=pltpu.VMEM)


def run_mixer(*operands):
    seq, model = operands[13].shape
    state = operands[1].shape
    part = model // PARTS
    out_rows = 128 * CAPACITY * PARTS
    return pl.pallas_call(
        mixer_kernel,
        in_specs=[pl.BlockSpec(memory_space=pltpu.HBM)] * MIXER_INS,
        out_specs=[pl.BlockSpec(memory_space=pltpu.HBM)] * 2 + [in_vmem()] * 3,
        out_shape=[
            pltpu.HBM(state, f32),
            pltpu.HBM(state, f32),
            jax.ShapeDtypeStruct((seq, model), bf16),
            jax.ShapeDtypeStruct((seq, model), bf16),
            jax.ShapeDtypeStruct((out_rows, part), bf16),
        ],
        scratch_shapes=[pltpu.VMEM(x.shape, x.dtype) for x in operands]
        + [
            pltpu.VMEM(state, f32),
            pltpu.VMEM(state, f32),
            pltpu.VMEM((out_rows, PARTS * seq), bf16),
            pltpu.VMEM((4, 256, 256), f32),
            pltpu.VMEM((4, 256, 256), f32),
            pltpu.VMEM((4, 256, 256), bf16),
            pltpu.VMEM((4, 256, 256), bf16),
            pltpu.SemaphoreType.DMA((13,)),
            pltpu.SemaphoreType.DMA((8,)),
            pltpu.SemaphoreType.DMA((2,)),
            pltpu.SemaphoreType.DMA((8,)),
        ],
        compiler_params=pltpu.CompilerParams(vmem_limit_bytes=28 << 20),
        name="mixer",
    )(*map(in_hbm, operands))


def swap_matrix(back):
    i = iota((CHUNK, CHUNK), 1 if back else 0)
    j = iota((CHUNK, CHUNK), 0 if back else 1)
    source = ((i // 4) % 16) * 16 + (i // 64) * 4 + i % 4
    return jnp.where(source == j, 1.0, 0.0).astype(bf16)


def expert_kernel(y_ref, wg_ref, wu_ref, wd_ref, z_ref, x_ref, h_ref, held, sems):
    model = wg_ref.shape[0]
    part = model // PARTS
    take = CHUNK // PARTS
    order = swap_matrix(False)
    chunks = y_ref.shape[0] // CHUNK
    for c in range(chunks):
        x = dot(order, y_ref[CHUNK * c : CHUNK * (c + 1), :]).astype(bf16)
        for q in range(PARTS):
            x_ref[take * c : take * (c + 1), part * q : part * (q + 1)] = x[take * q : take * (q + 1)]
    gate = dot(x_ref[...], wg_ref[...])
    up = dot(x_ref[...], wu_ref[...])
    h_ref[...] = (gate * jax.nn.sigmoid(gate) * up).astype(bf16)
    back = swap_matrix(True)
    halves = 2
    rows = h_ref.shape[0] // halves
    copies = []
    for h in range(halves):
        out = dot(h_ref[rows * h : rows * (h + 1), :], wd_ref[...]).astype(bf16)
        for c in range(rows // take):
            o = out[take * c : take * (c + 1)]
            o = jnp.concatenate([o[:, part * q : part * (q + 1)] for q in range(PARTS)], axis=0)
            first = PARTS * rows * h + CHUNK * c
            held[first : first + CHUNK, :] = dot(back, o).astype(bf16)
            span = pl.ds(first, CHUNK)
            copy = pltpu.make_async_copy(held.at[span], z_ref.at[span], sems.at[first // CHUNK])
            copy.start()
            copies.append(copy)
    for copy in copies:
        copy.wait()


def run_expert(y, wg, wu, wd):
    rows = y.shape[0] // PARTS
    return pl.pallas_call(
        expert_kernel,
        in_specs=[in_vmem()] * 4,
        out_specs=pl.BlockSpec(memory_space=pltpu.HBM),
        out_shape=pltpu.HBM(y.shape, bf16),
        scratch_shapes=[
            pltpu.VMEM((rows, wg.shape[0]), bf16),
            pltpu.VMEM((rows, wg.shape[1]), bf16),
            pltpu.VMEM(y.shape, bf16),
            pltpu.SemaphoreType.DMA((y.shape[0] // CHUNK,)),
        ],
        compiler_params=pltpu.CompilerParams(vmem_limit_bytes=20 << 20),
        name="expert",
    )(y, wg, wu, wd)


def shared_kernel(normed_ref, wg_ref, wu_ref, wd_ref, routes_ref, weights_ref, out_ref, mix_ref):
    x = normed_ref[...]
    gate = dot(x, wg_ref[...])
    up = dot(x, wu_ref[...])
    hidden = (gate * jax.nn.sigmoid(gate) * up).astype(bf16)
    out_ref[...] = dot(hidden, wd_ref[...])

    routes = routes_ref[...]
    weights = weights_ref[...]
    top, seq = routes.shape
    code = route_code(routes)
    row = iota(code.shape, 0)
    weight = jnp.zeros(code.shape, f32)
    for k in range(top):
        weight = weight + jnp.where(row == routes[k : k + 1, :], weights[k : k + 1, :], 0.0)
    slot = (iota((CHUNK, seq), 0) % CAPACITY).astype(f32)
    for c in range(mix_ref.shape[1] // CHUNK):
        r = slice(16 * c, 16 * (c + 1))
        hit = spread_rows(code[r]) == slot
        mix_ref[:, CHUNK * c : CHUNK * (c + 1)] = (
            jnp.where(hit, spread_rows(weight[r]), 0.0).T.astype(bf16)
        )


def run_shared(normed, wg, wu, wd, routes, weights):
    seq, model = normed.shape
    return pl.pallas_call(
        shared_kernel,
        out_shape=[
            jax.ShapeDtypeStruct((seq, model), f32),
            jax.ShapeDtypeStruct((seq, 128 * CAPACITY * PARTS), bf16),
        ],
        in_specs=[in_vmem()] * 6,
        out_specs=[in_vmem()] * 2,
        compiler_params=pltpu.CompilerParams(vmem_limit_bytes=16 << 20),
        cost_estimate=pl.CostEstimate(
            flops=2 * seq * model * wg.shape[1] * 60, bytes_accessed=8 << 20, transcendentals=0
        ),
        name="shared",
    )(normed, wg, wu, wd, routes, weights)


def combine_kernel(z_ref, mix_ref, shared_ref, mid_ref, gain_ref, out_ref):
    seq = mid_ref.shape[0]
    mix = mix_ref[...]
    part_of = (iota((1, mix.shape[1]), 1) // CAPACITY) % PARTS
    rows = [mix * jnp.where(part_of == q, 1.0, 0.0).astype(bf16) for q in range(PARTS)]
    both = dot(jnp.concatenate(rows, axis=0), z_ref[...])
    routed = jnp.concatenate([both[seq * q : seq * (q + 1)] for q in range(PARTS)], axis=1)
    combined = shared_ref[...] + routed
    out_ref[...] = (
        mid_ref[...].astype(f32) + combined * rms_scale(combined) * gain_ref[...]
    ).astype(bf16)


def run_combine(z, mix, shared, mid, gain):
    return pl.pallas_call(
        combine_kernel,
        out_shape=jax.ShapeDtypeStruct(mid.shape, bf16),
        in_specs=[in_vmem()] * 5,
        out_specs=in_vmem(),
        compiler_params=pltpu.CompilerParams(vmem_limit_bytes=16 << 20),
        name="combine",
    )(z, mix, shared, mid, gain)


def per_device(
    residual, branch_in, state_real, state_imag, decay_rate, frequency, log_step, input_real,
    input_imag, output_matrix_real, output_matrix_imaginary, skip_gain, glu_value, glu_gate,
    mix_gain, moe_in_gain, moe_out_gain, routes, route_weights, expert_gate, expert_up,
    expert_down, shared_gate, shared_up, shared_down,
):
    states = decay_rate.shape[1]
    model = residual.shape[1]
    part = model // PARTS
    row = lambda v: v.reshape(1, -1)
    inr = jnp.transpose(input_real, (0, 2, 1)).reshape(-1, states)
    ini = jnp.transpose(input_imag, (0, 2, 1)).reshape(-1, states)
    cr = output_matrix_real.reshape(-1, states)
    ci = output_matrix_imaginary.reshape(-1, states)
    routes_t = routes.T
    weights_t = route_weights.T
    next_real, next_imag, mid, normed, outgoing = run_mixer(
        branch_in, state_real, state_imag, decay_rate, frequency, row(log_step), inr, ini, cr, ci,
        row(skip_gain), glu_value, glu_gate, residual, row(mix_gain), row(moe_in_gain), routes_t,
    )

    def exchange(x):
        x = x.reshape(128, PARTS * CAPACITY, part)
        return lax.all_to_all(x, "ep", split_axis=0, concat_axis=0, tiled=True).reshape(-1, part)

    arrived = exchange(outgoing)
    shared, mix = run_shared(normed, shared_gate, shared_up, shared_down, routes_t, weights_t)
    returned = exchange(run_expert(arrived, expert_gate[0], expert_up[0], expert_down[0]))
    layer_out = run_combine(returned, mix, shared, mid, row(moe_out_gain))
    return layer_out, next_real, next_imag


def solution(mesh):
    rows2 = P("ep", None)
    rows3 = P("ep", None, None)
    return jax.shard_map(
        per_device,
        mesh=mesh,
        in_specs=(rows2,) * 4 + (P(),) * 13 + (rows2,) * 2 + (rows3,) * 3 + (P(),) * 3,
        out_specs=(rows2, rows2, rows2),
        check_vma=False,
    )
```

```python
import functools

import jax
import jax.numpy as jnp
from jax import lax
from jax.experimental import pallas as pl
from jax.experimental.pallas import tpu as pltpu
from jax.sharding import PartitionSpec as P

norm_eps = 1e-06
f32 = jnp.float32
bf16 = jnp.bfloat16

EXPERTS = 128
CAPACITY = 4


def iota(shape, dim):
    return lax.broadcasted_iota(jnp.int32, shape, dim)


def dot(a, b):
    return jnp.dot(a, b, preferred_element_type=f32)


def sin_cos(x):
    turns = jnp.floor(x * 0.6366197723675814 + 0.5)
    r = ((x - turns * 1.5703125) - turns * 4.837512969970703125e-4) - turns * 7.54978995489188216e-8
    z = r * r
    s = r + r * z * ((-1.9515295891e-4 * z + 8.3321608736e-3) * z - 1.6666654611e-1)
    c = 1.0 - 0.5 * z + z * z * (
        (2.443315711809948e-5 * z - 1.388731625493765e-3) * z + 4.166664568298827e-2
    )
    quarter = turns.astype(jnp.int32) & 3
    odd = (quarter & 1) == 1
    sin_x = jnp.where(odd, c, s)
    cos_x = jnp.where(odd, s, c)
    sin_x = jnp.where(quarter >= 2, -sin_x, sin_x)
    cos_x = jnp.where((quarter == 1) | (quarter == 2), -cos_x, cos_x)
    return sin_x, cos_x


def split(x):
    hi = x.astype(bf16)
    return hi, (x - hi.astype(f32)).astype(bf16)


def route_code(routes):
    top, seq = routes.shape
    row = iota((EXPERTS, seq), 0)
    named = jnp.zeros((EXPERTS, seq), f32)
    for k in range(top):
        named = named + jnp.where(row == routes[k : k + 1, :], 1.0, 0.0)
    before = jnp.where(iota((seq, seq), 0) < iota((seq, seq), 1), 1.0, 0.0).astype(bf16)
    rank = dot(named.astype(bf16), before)
    return jnp.where(named > 0.5, rank, -1.0)


def spread_rows(block):
    n = block.shape[0]
    one_hot = iota((CAPACITY * n, n), 0) // CAPACITY == iota((CAPACITY * n, n), 1)
    return dot(jnp.where(one_hot, 1.0, 0.0).astype(bf16), block.astype(bf16))


def slot_of_row(shape):
    return (iota(shape, 0) % CAPACITY).astype(f32)


def rms_scale(x):
    return lax.rsqrt(jnp.mean(x * x, axis=-1, keepdims=True) + norm_eps)


MIXER_INS = 17


def mixer_kernel(*refs):
    hbm = refs[:MIXER_INS]
    nr_ref, ni_ref, mid_ref, normed_ref, out_ref = refs[MIXER_INS : MIXER_INS + 5]
    local = refs[MIXER_INS + 5 : 2 * MIXER_INS + 5]
    nr, ni, select, force_re, force_im, read_re, read_im, small_sems, state_sems, glu_sems, out_sems = refs[2 * MIXER_INS + 5 :]
    (u_v, sr, si, decay_v, freq_v, log_v, inr, ini, cr, ci,
     skip_v, gv, gg, res_v, mix_v, gain_v, routes_v) = local

    def copies_of(index, count, axis, sems, first):
        size = hbm[index].shape[axis] // count
        made = []
        for k in range(count):
            span = pl.ds(size * k, size)
            at = (slice(None), span) if axis else (span, slice(None))
            made.append(
                pltpu.make_async_copy(hbm[index].at[at], local[index].at[at], sems.at[first + k])
            )
        return made

    cuts = 4
    small = {}
    for n, index in enumerate((3, 4, 5, 16, 0, 6, 7, 8, 9, 10, 13, 14, 15)):
        small[index] = copies_of(index, 1, 0, small_sems, n)[0]
    state = [copies_of(1, cuts, 1, state_sems, 0), copies_of(2, cuts, 1, state_sems, cuts)]
    glu_cuts = glu_sems.shape[0] // 2
    value = copies_of(11, glu_cuts, 1, glu_sems, 0)
    gate = copies_of(12, glu_cuts, 1, glu_sems, glu_cuts)
    for index in (3, 4, 5, 16, 0, 6, 7, 8, 9, 10):
        small[index].start()
    for j in range(cuts):
        state[0][j].start()
        state[1][j].start()
    for n in range(glu_cuts):
        value[n].start()
        gate[n].start()
    for index in (13, 14, 15):
        small[index].start()

    seq = u_v.shape[0]
    groups, states = decay_v.shape
    packed = 4
    wide = packed * states
    cols = u_v.shape[1] // cuts
    chans = cols // (groups // cuts)

    small[16].wait()
    code = spread_rows(route_code(routes_v[...]))
    select[...] = jnp.where(code == slot_of_row(code.shape), 1.0, 0.0).astype(bf16)

    small[5].wait()
    small[3].wait()
    small[4].wait()
    pick = iota((groups, groups), 1) == iota((groups, groups), 0)
    step_size = jnp.exp(jnp.sum(jnp.where(pick, log_v[...], 0.0), axis=1, keepdims=True))
    decay = decay_v[...]
    freq = freq_v[...]
    magnitude = jnp.exp(-decay * step_size)
    sin_x, cos_x = sin_cos(freq * step_size)
    a_re = magnitude * cos_x
    a_im = magnitude * sin_x
    lam = -decay
    den = lam * lam + freq * freq
    num = a_re - 1.0
    k_re = (num * lam + a_im * freq) / den
    k_im = (a_im * lam - num * freq) / den
    own = iota((groups, wide), 0) % packed == iota((groups, wide), 1) // states

    def tiled(x):
        twice = jnp.concatenate([x, x], axis=1)
        return jnp.concatenate([twice] * (packed // 2), axis=1)

    def flat(x):
        x = jnp.where(own, tiled(x), 0.0)
        return [
            jnp.sum(x[packed * b : packed * (b + 1)], axis=0, keepdims=True)
            for b in range(groups // packed)
        ]

    a_re, a_im, k_re, k_im = flat(a_re), flat(a_im), flat(k_re), flat(k_im)

    patch = (iota((cols, wide), 0) // chans) % packed == iota((cols, wide), 1) // states

    def weights(ref, j):
        x = ref[cols * j : cols * (j + 1), :].astype(f32)
        return jnp.where(patch, tiled(x), 0.0).astype(bf16)

    lane = iota((seq, cols), 1) // (cols // packed)
    for index in (0, 6, 7):
        small[index].wait()
    for j in range(cuts):
        u = u_v[:, cols * j : cols * (j + 1)].astype(f32)
        spread = jnp.concatenate(
            [jnp.where(lane == k, u, 0.0) for k in range(packed)], axis=0
        ).astype(bf16)
        force_re[j] = dot(spread, weights(inr, j))
        force_im[j] = dot(spread, weights(ini, j))
    for index in (8, 9, 10):
        small[index].wait()
    for j in range(cuts):
        read_re[j] = weights(cr, j)
        read_im[j] = weights(ci, j)

    outs = []
    acts = []
    for j in range(cuts):
        u = u_v[:, cols * j : cols * (j + 1)].astype(f32)
        f_re = force_re[j]
        f_im = force_im[j]
        state[0][j].wait()
        state[1][j].wait()
        fresh_re, fresh_im = [], []
        for k in range(packed):
            b = packed * j + k
            at = slice(wide * b, wide * (b + 1))
            r = slice(seq * k, seq * (k + 1))
            old_re = sr[:, at]
            old_im = si[:, at]
            new_re = a_re[b] * old_re - a_im[b] * old_im + (k_re[b] * f_re[r] - k_im[b] * f_im[r])
            new_im = a_re[b] * old_im + a_im[b] * old_re + (k_re[b] * f_im[r] + k_im[b] * f_re[r])
            nr[:, at] = new_re
            ni[:, at] = new_im
            fresh_re.append(new_re)
            fresh_im.append(new_im)
        for n, (src, dst) in enumerate(((nr, nr_ref), (ni, ni_ref))):
            at = (slice(None), pl.ds(packed * wide * j, packed * wide))
            copy = pltpu.make_async_copy(src.at[at], dst.at[at], out_sems.at[cuts * n + j])
            outs.append(copy)

        def read(parts, ref):
            pairs = [split(x) for x in parts]
            rows = jnp.concatenate([p[0] for p in pairs] + [p[1] for p in pairs], axis=0)
            got = lax.dot_general(
                rows, ref[j], (((1,), (1,)), ((), ())), preferred_element_type=f32
            )
            return got[: packed * seq] + got[packed * seq :]

        both = read(fresh_re, read_re) - read(fresh_im, read_im)
        readout = both[:seq]
        for k in range(1, packed):
            readout = jnp.where(lane == k, both[seq * k : seq * (k + 1)], readout)
        mixed = readout + skip_v[:, cols * j : cols * (j + 1)] * u
        acts.append(jax.nn.gelu(mixed).astype(bf16))

    act = jnp.concatenate(acts, axis=1)
    piece = gv.shape[1] // glu_cuts
    pieces = []
    for n in range(glu_cuts):
        at = slice(piece * n, piece * (n + 1))
        value[n].wait()
        value_part = dot(act, gv[:, at])
        gate[n].wait()
        if n == glu_cuts - 1:
            for copy in outs:
                copy.start()
        pieces.append(value_part * jax.nn.sigmoid(dot(act, gg[:, at])))
    branch = jnp.concatenate(pieces, axis=1)
    for index in (13, 14, 15):
        small[index].wait()
    mid = (res_v[...].astype(f32) + branch * rms_scale(branch) * mix_v[...]).astype(bf16)
    mid_ref[...] = mid
    mid = mid.astype(f32)
    normed = (mid * rms_scale(mid) * gain_v[...]).astype(bf16)
    normed_ref[...] = normed
    width = 512
    for n in range(normed.shape[1] // width):
        at = slice(width * n, width * (n + 1))
        rows = dot(select[...], normed[:, at]).astype(bf16)
        out_ref[:, :, at] = rows.reshape(EXPERTS, CAPACITY, width)
    for copy in outs:
        copy.wait()


def in_hbm(x):
    return pltpu.with_memory_space_constraint(x, pltpu.HBM)


def in_vmem():
    return pl.BlockSpec(memory_space=pltpu.VMEM)


def run_mixer(*operands):
    seq, model = operands[13].shape
    state = operands[1].shape
    return pl.pallas_call(
        mixer_kernel,
        in_specs=[pl.BlockSpec(memory_space=pltpu.HBM)] * MIXER_INS,
        out_specs=[pl.BlockSpec(memory_space=pltpu.HBM)] * 2 + [in_vmem()] * 3,
        out_shape=[
            pltpu.HBM(state, f32),
            pltpu.HBM(state, f32),
            jax.ShapeDtypeStruct((seq, model), bf16),
            jax.ShapeDtypeStruct((seq, model), bf16),
            jax.ShapeDtypeStruct((EXPERTS, CAPACITY, model), bf16),
        ],
        scratch_shapes=[pltpu.VMEM(x.shape, x.dtype) for x in operands]
        + [
            pltpu.VMEM(state, f32),
            pltpu.VMEM(state, f32),
            pltpu.VMEM((EXPERTS * CAPACITY, seq), bf16),
            pltpu.VMEM((4, 256, 256), f32),
            pltpu.VMEM((4, 256, 256), f32),
            pltpu.VMEM((4, 256, 256), bf16),
            pltpu.VMEM((4, 256, 256), bf16),
            pltpu.SemaphoreType.DMA((13,)),
            pltpu.SemaphoreType.DMA((8,)),
            pltpu.SemaphoreType.DMA((2,)),
            pltpu.SemaphoreType.DMA((8,)),
        ],
        compiler_params=pltpu.CompilerParams(vmem_limit_bytes=28 << 20),
        name="mixer",
    )(*map(in_hbm, operands))


def expert_kernel(
    y_ref, wg_ref, wu_ref, wd_hbm, z_ref, x_ref, h_ref, wd_ref, held, sems, wd_sem
):
    wd_copy = pltpu.make_async_copy(wd_hbm, wd_ref, wd_sem.at[0])
    wd_copy.start()
    senders, slots, model = y_ref.shape
    x_ref[...] = y_ref[...].reshape(x_ref.shape)
    gate = dot(x_ref[...], wg_ref[...])
    up = dot(x_ref[...], wu_ref[...])
    h_ref[...] = (gate * jax.nn.sigmoid(gate) * up).astype(bf16)
    wd_copy.wait()
    halves = sems.shape[0]
    some = senders // halves
    copies = []
    for h in range(halves):
        out = dot(h_ref[slots * some * h : slots * some * (h + 1), :], wd_ref[...]).astype(bf16)
        held[some * h : some * (h + 1)] = out.reshape(some, slots, model)
        span = pl.ds(some * h, some)
        copy = pltpu.make_async_copy(held.at[span], z_ref.at[span], sems.at[h])
        copy.start()
        copies.append(copy)
    for copy in copies:
        copy.wait()


def run_expert(y, wg, wu, wd):
    rows = y.shape[0] * y.shape[1]
    return pl.pallas_call(
        expert_kernel,
        in_specs=[in_vmem()] * 3 + [pl.BlockSpec(memory_space=pltpu.HBM)],
        out_specs=pl.BlockSpec(memory_space=pltpu.HBM),
        out_shape=pltpu.HBM(y.shape, bf16),
        scratch_shapes=[
            pltpu.VMEM((rows, wg.shape[0]), bf16),
            pltpu.VMEM((rows, wg.shape[1]), bf16),
            pltpu.VMEM(wd.shape, bf16),
            pltpu.VMEM(y.shape, bf16),
            pltpu.SemaphoreType.DMA((2,)),
            pltpu.SemaphoreType.DMA((1,)),
        ],
        compiler_params=pltpu.CompilerParams(vmem_limit_bytes=20 << 20),
        name="expert",
    )(y, wg, wu, in_hbm(wd))


def shared_kernel(normed_ref, wg_ref, wu_ref, wd_ref, routes_ref, weights_ref, out_ref, mix_ref):
    x = normed_ref[...]
    gate = dot(x, wg_ref[...])
    up = dot(x, wu_ref[...])
    hidden = (gate * jax.nn.sigmoid(gate) * up).astype(bf16)
    out_ref[...] = dot(hidden, wd_ref[...])

    routes = routes_ref[...]
    weights = weights_ref[...]
    top, seq = routes.shape
    code = route_code(routes)
    row = iota(code.shape, 0)
    weight = jnp.zeros(code.shape, f32)
    for k in range(top):
        weight = weight + jnp.where(row == routes[k : k + 1, :], weights[k : k + 1, :], 0.0)
    code = spread_rows(code)
    hit = code == slot_of_row(code.shape)
    hi, lo = split(weight)
    for h, w in enumerate((hi, lo)):
        mix_ref[seq * h : seq * (h + 1), :] = jnp.where(hit, spread_rows(w), 0.0).T.astype(bf16)


def run_shared(normed, wg, wu, wd, routes, weights):
    seq, model = normed.shape
    return pl.pallas_call(
        shared_kernel,
        out_shape=[
            jax.ShapeDtypeStruct((seq, model), f32),
            jax.ShapeDtypeStruct((2 * seq, EXPERTS * CAPACITY), bf16),
        ],
        in_specs=[in_vmem()] * 6,
        out_specs=[in_vmem()] * 2,
        compiler_params=pltpu.CompilerParams(vmem_limit_bytes=16 << 20),
        cost_estimate=pl.CostEstimate(
            flops=2 * seq * model * wg.shape[1] * 60, bytes_accessed=8 << 20, transcendentals=0
        ),
        name="shared",
    )(normed, wg, wu, wd, routes, weights)


def combine_kernel(z_ref, mix_ref, shared_ref, mid_ref, gain_ref, out_ref):
    seq = mid_ref.shape[0]
    both = dot(mix_ref[...], z_ref[...].reshape(mix_ref.shape[1], out_ref.shape[1]))
    routed = both[:seq] + both[seq:]
    combined = shared_ref[...] + routed
    out_ref[...] = (
        mid_ref[...].astype(f32) + combined * rms_scale(combined) * gain_ref[...]
    ).astype(bf16)


def run_combine(z, mix, shared, mid, gain):
    return pl.pallas_call(
        combine_kernel,
        out_shape=jax.ShapeDtypeStruct(mid.shape, bf16),
        in_specs=[in_vmem()] * 5,
        out_specs=in_vmem(),
        compiler_params=pltpu.CompilerParams(vmem_limit_bytes=16 << 20),
        name="combine",
    )(z, mix, shared, mid, gain)


def per_device(
    residual, branch_in, state_real, state_imag, decay_rate, frequency, log_step, input_real,
    input_imag, output_matrix_real, output_matrix_imaginary, skip_gain, glu_value, glu_gate,
    mix_gain, moe_in_gain, moe_out_gain, routes, route_weights, expert_gate, expert_up,
    expert_down, shared_gate, shared_up, shared_down,
):
    states = decay_rate.shape[1]
    row = lambda v: v.reshape(1, -1)
    inr = jnp.transpose(input_real, (0, 2, 1)).reshape(-1, states)
    ini = jnp.transpose(input_imag, (0, 2, 1)).reshape(-1, states)
    cr = output_matrix_real.reshape(-1, states)
    ci = output_matrix_imaginary.reshape(-1, states)
    routes_t = routes.T
    weights_t = route_weights.T
    next_real, next_imag, mid, normed, outgoing = run_mixer(
        branch_in, state_real, state_imag, decay_rate, frequency, row(log_step), inr, ini, cr, ci,
        row(skip_gain), glu_value, glu_gate, residual, row(mix_gain), row(moe_in_gain), routes_t,
    )

    def exchange(x):
        return lax.all_to_all(x, "ep", split_axis=0, concat_axis=0, tiled=True)

    arrived = exchange(outgoing)
    shared, mix = run_shared(normed, shared_gate, shared_up, shared_down, routes_t, weights_t)
    returned = exchange(run_expert(arrived, expert_gate[0], expert_up[0], expert_down[0]))
    layer_out = run_combine(returned, mix, shared, mid, row(moe_out_gain))
    return layer_out, next_real, next_imag


def solution(mesh):
    rows2 = P("ep", None)
    rows3 = P("ep", None, None)
    return jax.shard_map(
        per_device,
        mesh=mesh,
        in_specs=(rows2,) * 4 + (P(),) * 13 + (rows2,) * 2 + (rows3,) * 3 + (P(),) * 3,
        out_specs=(rows2, rows2, rows2),
        check_vma=False,
    )
```

```python
import functools

import jax
import jax.numpy as jnp
from jax import lax
from jax.experimental import pallas as pl
from jax.experimental.pallas import tpu as pltpu
from jax.sharding import PartitionSpec as P

norm_eps = 1e-06
f32 = jnp.float32
bf16 = jnp.bfloat16

EXPERTS = 128
CAPACITY = 4


def iota(shape, dim):
    return lax.broadcasted_iota(jnp.int32, shape, dim)


def dot(a, b):
    return jnp.dot(a, b, preferred_element_type=f32)


def sin_cos(x):
    turns = jnp.floor(x * 0.6366197723675814 + 0.5)
    r = ((x - turns * 1.5703125) - turns * 4.837512969970703125e-4) - turns * 7.54978995489188216e-8
    z = r * r
    s = r + r * z * ((-1.9515295891e-4 * z + 8.3321608736e-3) * z - 1.6666654611e-1)
    c = 1.0 - 0.5 * z + z * z * (
        (2.443315711809948e-5 * z - 1.388731625493765e-3) * z + 4.166664568298827e-2
    )
    quarter = turns.astype(jnp.int32) & 3
    odd = (quarter & 1) == 1
    sin_x = jnp.where(odd, c, s)
    cos_x = jnp.where(odd, s, c)
    sin_x = jnp.where(quarter >= 2, -sin_x, sin_x)
    cos_x = jnp.where((quarter == 1) | (quarter == 2), -cos_x, cos_x)
    return sin_x, cos_x


def split(x):
    hi = x.astype(bf16)
    return hi, (x - hi.astype(f32)).astype(bf16)


def route_code(routes):
    top, seq = routes.shape
    row = iota((EXPERTS, seq), 0)
    named = jnp.zeros((EXPERTS, seq), f32)
    for k in range(top):
        named = named + jnp.where(row == routes[k : k + 1, :], 1.0, 0.0)
    before = jnp.where(iota((seq, seq), 0) < iota((seq, seq), 1), 1.0, 0.0).astype(bf16)
    rank = dot(named.astype(bf16), before)
    return jnp.where(named > 0.5, rank, -1.0)


def spread_rows(block):
    n = block.shape[0]
    one_hot = iota((CAPACITY * n, n), 0) // CAPACITY == iota((CAPACITY * n, n), 1)
    return dot(jnp.where(one_hot, 1.0, 0.0).astype(bf16), block.astype(bf16))


def slot_of_row(shape):
    return (iota(shape, 0) % CAPACITY).astype(f32)


def rms_scale(x):
    return lax.rsqrt(jnp.mean(x * x, axis=-1, keepdims=True) + norm_eps)


MIXER_INS = 17


def mixer_kernel(*refs):
    hbm = refs[:MIXER_INS]
    nr_ref, ni_ref, mid_ref, normed_ref, out_ref = refs[MIXER_INS : MIXER_INS + 5]
    local = refs[MIXER_INS + 5 : 2 * MIXER_INS + 5]
    nr, ni, select, force_re, force_im, read_re, read_im, small_sems, state_sems, glu_sems, out_sems = refs[2 * MIXER_INS + 5 :]
    (u_v, sr, si, decay_v, freq_v, log_v, inr, ini, cr, ci,
     skip_v, gv, gg, res_v, mix_v, gain_v, routes_v) = local

    def copies_of(index, count, axis, sems, first):
        size = hbm[index].shape[axis] // count
        made = []
        for k in range(count):
            span = pl.ds(size * k, size)
            at = (slice(None), span) if axis else (span, slice(None))
            made.append(
                pltpu.make_async_copy(hbm[index].at[at], local[index].at[at], sems.at[first + k])
            )
        return made

    cuts = 4
    small = {}
    for n, index in enumerate((3, 4, 5, 16, 0, 6, 7, 8, 9, 10, 13, 14, 15)):
        small[index] = copies_of(index, 1, 0, small_sems, n)[0]
    state = [copies_of(1, cuts, 1, state_sems, 0), copies_of(2, cuts, 1, state_sems, cuts)]
    glu_cuts = glu_sems.shape[0] // 2
    value = copies_of(11, glu_cuts, 1, glu_sems, 0)
    gate = copies_of(12, glu_cuts, 1, glu_sems, glu_cuts)
    for index in (3, 4, 5, 16, 0, 6, 7, 8, 9, 10):
        small[index].start()
    for j in range(cuts):
        state[0][j].start()
        state[1][j].start()
    for n in range(glu_cuts):
        value[n].start()
        gate[n].start()
    for index in (13, 14, 15):
        small[index].start()

    seq = u_v.shape[0]
    groups, states = decay_v.shape
    packed = 4
    wide = packed * states
    cols = u_v.shape[1] // cuts
    chans = cols // (groups // cuts)

    small[16].wait()
    code = spread_rows(route_code(routes_v[...]))
    select[...] = jnp.where(code == slot_of_row(code.shape), 1.0, 0.0).astype(bf16)

    small[5].wait()
    small[3].wait()
    small[4].wait()
    pick = iota((groups, groups), 1) == iota((groups, groups), 0)
    step_size = jnp.exp(jnp.sum(jnp.where(pick, log_v[...], 0.0), axis=1, keepdims=True))
    decay = decay_v[...]
    freq = freq_v[...]
    magnitude = jnp.exp(-decay * step_size)
    sin_x, cos_x = sin_cos(freq * step_size)
    a_re = magnitude * cos_x
    a_im = magnitude * sin_x
    lam = -decay
    den = lam * lam + freq * freq
    num = a_re - 1.0
    k_re = (num * lam + a_im * freq) / den
    k_im = (a_im * lam - num * freq) / den
    own = iota((groups, wide), 0) % packed == iota((groups, wide), 1) // states

    def tiled(x):
        twice = jnp.concatenate([x, x], axis=1)
        return jnp.concatenate([twice] * (packed // 2), axis=1)

    def flat(x):
        x = jnp.where(own, tiled(x), 0.0)
        return [
            jnp.sum(x[packed * b : packed * (b + 1)], axis=0, keepdims=True)
            for b in range(groups // packed)
        ]

    a_re, a_im, k_re, k_im = flat(a_re), flat(a_im), flat(k_re), flat(k_im)

    patch = (iota((cols, wide), 0) // chans) % packed == iota((cols, wide), 1) // states

    def weights(ref, j):
        x = ref[cols * j : cols * (j + 1), :].astype(f32)
        return jnp.where(patch, tiled(x), 0.0).astype(bf16)

    lane = iota((seq, cols), 1) // (cols // packed)
    for index in (0, 6, 7):
        small[index].wait()
    for j in range(cuts):
        u = u_v[:, cols * j : cols * (j + 1)].astype(f32)
        spread = jnp.concatenate(
            [jnp.where(lane == k, u, 0.0) for k in range(packed)], axis=0
        ).astype(bf16)
        force_re[j] = dot(spread, weights(inr, j))
        force_im[j] = dot(spread, weights(ini, j))
    for index in (8, 9, 10):
        small[index].wait()
    for j in range(cuts):
        read_re[j] = weights(cr, j)
        read_im[j] = weights(ci, j)

    outs = []
    acts = []
    for j in range(cuts):
        u = u_v[:, cols * j : cols * (j + 1)].astype(f32)
        f_re = force_re[j]
        f_im = force_im[j]
        state[0][j].wait()
        state[1][j].wait()
        fresh_re, fresh_im = [], []
        for k in range(packed):
            b = packed * j + k
            at = slice(wide * b, wide * (b + 1))
            r = slice(seq * k, seq * (k + 1))
            old_re = sr[:, at]
            old_im = si[:, at]
            new_re = a_re[b] * old_re - a_im[b] * old_im + (k_re[b] * f_re[r] - k_im[b] * f_im[r])
            new_im = a_re[b] * old_im + a_im[b] * old_re + (k_re[b] * f_im[r] + k_im[b] * f_re[r])
            nr[:, at] = new_re
            ni[:, at] = new_im
            fresh_re.append(new_re)
            fresh_im.append(new_im)
        for n, (src, dst) in enumerate(((nr, nr_ref), (ni, ni_ref))):
            at = (slice(None), pl.ds(packed * wide * j, packed * wide))
            copy = pltpu.make_async_copy(src.at[at], dst.at[at], out_sems.at[cuts * n + j])
            outs.append(copy)

        def read(parts, ref):
            pairs = [split(x) for x in parts]
            rows = jnp.concatenate([p[0] for p in pairs] + [p[1] for p in pairs], axis=0)
            got = lax.dot_general(
                rows, ref[j], (((1,), (1,)), ((), ())), preferred_element_type=f32
            )
            return got[: packed * seq] + got[packed * seq :]

        both = read(fresh_re, read_re) - read(fresh_im, read_im)
        readout = both[:seq]
        for k in range(1, packed):
            readout = jnp.where(lane == k, both[seq * k : seq * (k + 1)], readout)
        mixed = readout + skip_v[:, cols * j : cols * (j + 1)] * u
        acts.append(jax.nn.gelu(mixed).astype(bf16))

    act = jnp.concatenate(acts, axis=1)
    piece = gv.shape[1] // glu_cuts
    pieces = []
    for n in range(glu_cuts):
        at = slice(piece * n, piece * (n + 1))
        value[n].wait()
        value_part = dot(act, gv[:, at])
        gate[n].wait()
        if n == glu_cuts - 1:
            for copy in outs:
                copy.start()
        pieces.append(value_part * jax.nn.sigmoid(dot(act, gg[:, at])))
    branch = jnp.concatenate(pieces, axis=1)
    for index in (13, 14, 15):
        small[index].wait()
    mid = (res_v[...].astype(f32) + branch * rms_scale(branch) * mix_v[...]).astype(bf16)
    mid_ref[...] = mid
    mid = mid.astype(f32)
    normed = (mid * rms_scale(mid) * gain_v[...]).astype(bf16)
    normed_ref[...] = normed
    width = 512
    for n in range(normed.shape[1] // width):
        at = slice(width * n, width * (n + 1))
        rows = dot(select[...], normed[:, at]).astype(bf16)
        out_ref[:, :, at] = rows.reshape(EXPERTS, CAPACITY, width)
    for copy in outs:
        copy.wait()


def in_hbm(x):
    return pltpu.with_memory_space_constraint(x, pltpu.HBM)


def in_vmem():
    return pl.BlockSpec(memory_space=pltpu.VMEM)


def run_mixer(*operands):
    seq, model = operands[13].shape
    state = operands[1].shape
    return pl.pallas_call(
        mixer_kernel,
        in_specs=[pl.BlockSpec(memory_space=pltpu.HBM)] * MIXER_INS,
        out_specs=[pl.BlockSpec(memory_space=pltpu.HBM)] * 2 + [in_vmem()] * 3,
        out_shape=[
            pltpu.HBM(state, f32),
            pltpu.HBM(state, f32),
            jax.ShapeDtypeStruct((seq, model), bf16),
            jax.ShapeDtypeStruct((seq, model), bf16),
            jax.ShapeDtypeStruct((EXPERTS, CAPACITY, model), bf16),
        ],
        scratch_shapes=[pltpu.VMEM(x.shape, x.dtype) for x in operands]
        + [
            pltpu.VMEM(state, f32),
            pltpu.VMEM(state, f32),
            pltpu.VMEM((EXPERTS * CAPACITY, seq), bf16),
            pltpu.VMEM((4, 256, 256), f32),
            pltpu.VMEM((4, 256, 256), f32),
            pltpu.VMEM((4, 256, 256), bf16),
            pltpu.VMEM((4, 256, 256), bf16),
            pltpu.SemaphoreType.DMA((13,)),
            pltpu.SemaphoreType.DMA((8,)),
            pltpu.SemaphoreType.DMA((2,)),
            pltpu.SemaphoreType.DMA((8,)),
        ],
        compiler_params=pltpu.CompilerParams(vmem_limit_bytes=28 << 20),
        name="mixer",
    )(*map(in_hbm, operands))


def expert_kernel(y_ref, wg_ref, wu_ref, wd_ref, z_ref, h_ref, held, sems):
    senders, slots, model = y_ref.shape
    x = y_ref[...].reshape(senders * slots, model)
    gate = dot(x, wg_ref[...])
    up = dot(x, wu_ref[...])
    h_ref[...] = (gate * jax.nn.sigmoid(gate) * up).astype(bf16)
    pieces = sems.shape[0]
    width = model // pieces
    copies = []
    for n in range(pieces):
        out = dot(h_ref[...], wd_ref[:, width * n : width * (n + 1)]).astype(bf16)
        held[:, :, width * n : width * (n + 1)] = out.reshape(senders, slots, width)
        at = (slice(None), slice(None), pl.ds(width * n, width))
        copy = pltpu.make_async_copy(held.at[at], z_ref.at[at], sems.at[n])
        copy.start()
        copies.append(copy)
    for copy in copies:
        copy.wait()


def run_expert(y, wg, wu, wd):
    rows = y.shape[0] * y.shape[1]
    return pl.pallas_call(
        expert_kernel,
        in_specs=[in_vmem()] * 4,
        out_specs=pl.BlockSpec(memory_space=pltpu.HBM),
        out_shape=pltpu.HBM(y.shape, bf16),
        scratch_shapes=[
            pltpu.VMEM((rows, wg.shape[1]), bf16),
            pltpu.VMEM(y.shape, bf16),
            pltpu.SemaphoreType.DMA((4,)),
        ],
        compiler_params=pltpu.CompilerParams(vmem_limit_bytes=20 << 20),
        name="expert",
    )(y, wg, wu, wd)


def shared_kernel(normed_ref, wg_ref, wu_ref, wd_ref, routes_ref, weights_ref, out_ref, mix_ref):
    x = normed_ref[...]
    gate = dot(x, wg_ref[...])
    up = dot(x, wu_ref[...])
    hidden = (gate * jax.nn.sigmoid(gate) * up).astype(bf16)
    out_ref[...] = dot(hidden, wd_ref[...])

    routes = routes_ref[...]
    weights = weights_ref[...]
    top, seq = routes.shape
    code = route_code(routes)
    row = iota(code.shape, 0)
    weight = jnp.zeros(code.shape, f32)
    for k in range(top):
        weight = weight + jnp.where(row == routes[k : k + 1, :], weights[k : k + 1, :], 0.0)
    code = spread_rows(code)
    hit = code == slot_of_row(code.shape)
    hi, lo = split(weight)
    for h, w in enumerate((hi, lo)):
        mix_ref[seq * h : seq * (h + 1), :] = jnp.where(hit, spread_rows(w), 0.0).T.astype(bf16)


def run_shared(normed, wg, wu, wd, routes, weights):
    seq, model = normed.shape
    return pl.pallas_call(
        shared_kernel,
        out_shape=[
            jax.ShapeDtypeStruct((seq, model), f32),
            jax.ShapeDtypeStruct((2 * seq, EXPERTS * CAPACITY), bf16),
        ],
        in_specs=[in_vmem()] * 6,
        out_specs=[in_vmem()] * 2,
        compiler_params=pltpu.CompilerParams(vmem_limit_bytes=16 << 20),
        cost_estimate=pl.CostEstimate(
            flops=2 * seq * model * wg.shape[1] * 60, bytes_accessed=8 << 20, transcendentals=0
        ),
        name="shared",
    )(normed, wg, wu, wd, routes, weights)


def combine_kernel(z_ref, mix_ref, shared_ref, mid_ref, gain_ref, out_ref):
    seq = mid_ref.shape[0]
    both = dot(mix_ref[...], z_ref[...].reshape(mix_ref.shape[1], out_ref.shape[1]))
    routed = both[:seq] + both[seq:]
    combined = shared_ref[...] + routed
    out_ref[...] = (
        mid_ref[...].astype(f32) + combined * rms_scale(combined) * gain_ref[...]
    ).astype(bf16)


def run_combine(z, mix, shared, mid, gain):
    return pl.pallas_call(
        combine_kernel,
        out_shape=jax.ShapeDtypeStruct(mid.shape, bf16),
        in_specs=[in_vmem()] * 5,
        out_specs=in_vmem(),
        compiler_params=pltpu.CompilerParams(vmem_limit_bytes=16 << 20),
        name="combine",
    )(z, mix, shared, mid, gain)


def per_device(
    residual, branch_in, state_real, state_imag, decay_rate, frequency, log_step, input_real,
    input_imag, output_matrix_real, output_matrix_imaginary, skip_gain, glu_value, glu_gate,
    mix_gain, moe_in_gain, moe_out_gain, routes, route_weights, expert_gate, expert_up,
    expert_down, shared_gate, shared_up, shared_down,
):
    states = decay_rate.shape[1]
    row = lambda v: v.reshape(1, -1)
    inr = jnp.transpose(input_real, (0, 2, 1)).reshape(-1, states)
    ini = jnp.transpose(input_imag, (0, 2, 1)).reshape(-1, states)
    cr = output_matrix_real.reshape(-1, states)
    ci = output_matrix_imaginary.reshape(-1, states)
    routes_t = routes.T
    weights_t = route_weights.T
    next_real, next_imag, mid, normed, outgoing = run_mixer(
        branch_in, state_real, state_imag, decay_rate, frequency, row(log_step), inr, ini, cr, ci,
        row(skip_gain), glu_value, glu_gate, residual, row(mix_gain), row(moe_in_gain), routes_t,
    )

    def exchange(x):
        return lax.all_to_all(x, "ep", split_axis=0, concat_axis=0, tiled=True)

    arrived = exchange(outgoing)
    shared, mix = run_shared(normed, shared_gate, shared_up, shared_down, routes_t, weights_t)
    returned = exchange(run_expert(arrived, expert_gate[0], expert_up[0], expert_down[0]))
    layer_out = run_combine(returned, mix, shared, mid, row(moe_out_gain))
    return layer_out, next_real, next_imag


def solution(mesh):
    rows2 = P("ep", None)
    rows3 = P("ep", None, None)
    return jax.shard_map(
        per_device,
        mesh=mesh,
        in_specs=(rows2,) * 4 + (P(),) * 13 + (rows2,) * 2 + (rows3,) * 3 + (P(),) * 3,
        out_specs=(rows2, rows2, rows2),
        check_vma=False,
    )
```

```python
import functools

import jax
import jax.numpy as jnp
from jax import lax
from jax.experimental import pallas as pl
from jax.experimental.pallas import tpu as pltpu
from jax.sharding import PartitionSpec as P

norm_eps = 1e-06
f32 = jnp.float32
bf16 = jnp.bfloat16

EXPERTS = 128
CAPACITY = 4


def iota(shape, dim):
    return lax.broadcasted_iota(jnp.int32, shape, dim)


def dot(a, b):
    return jnp.dot(a, b, preferred_element_type=f32)


def sin_cos(x):
    turns = jnp.floor(x * 0.6366197723675814 + 0.5)
    r = ((x - turns * 1.5703125) - turns * 4.837512969970703125e-4) - turns * 7.54978995489188216e-8
    z = r * r
    s = r + r * z * ((-1.9515295891e-4 * z + 8.3321608736e-3) * z - 1.6666654611e-1)
    c = 1.0 - 0.5 * z + z * z * (
        (2.443315711809948e-5 * z - 1.388731625493765e-3) * z + 4.166664568298827e-2
    )
    quarter = turns.astype(jnp.int32) & 3
    odd = (quarter & 1) == 1
    sin_x = jnp.where(odd, c, s)
    cos_x = jnp.where(odd, s, c)
    sin_x = jnp.where(quarter >= 2, -sin_x, sin_x)
    cos_x = jnp.where((quarter == 1) | (quarter == 2), -cos_x, cos_x)
    return sin_x, cos_x


def split(x):
    hi = x.astype(bf16)
    return hi, (x - hi.astype(f32)).astype(bf16)


def route_code(routes):
    top, seq = routes.shape
    row = iota((EXPERTS, seq), 0)
    named = jnp.zeros((EXPERTS, seq), f32)
    for k in range(top):
        named = named + jnp.where(row == routes[k : k + 1, :], 1.0, 0.0)
    before = jnp.where(iota((seq, seq), 0) < iota((seq, seq), 1), 1.0, 0.0).astype(bf16)
    rank = dot(named.astype(bf16), before)
    return jnp.where(named > 0.5, rank, -1.0)


def spread_rows(block):
    n = block.shape[0]
    one_hot = iota((CAPACITY * n, n), 0) // CAPACITY == iota((CAPACITY * n, n), 1)
    return dot(jnp.where(one_hot, 1.0, 0.0).astype(bf16), block.astype(bf16))


def slot_of_row(shape):
    return (iota(shape, 0) % CAPACITY).astype(f32)


def rms_scale(x):
    return lax.rsqrt(jnp.mean(x * x, axis=-1, keepdims=True) + norm_eps)


MIXER_INS = 17


def mixer_kernel(*refs):
    hbm = refs[:MIXER_INS]
    nr_ref, ni_ref, mid_ref, normed_ref, out_ref = refs[MIXER_INS : MIXER_INS + 5]
    local = refs[MIXER_INS + 5 : 2 * MIXER_INS + 5]
    nr, ni, select, force_re, force_im, read_re, read_im, small_sems, state_sems, glu_sems, out_sems = refs[2 * MIXER_INS + 5 :]
    (u_v, sr, si, decay_v, freq_v, log_v, inr, ini, cr, ci,
     skip_v, gv, gg, res_v, mix_v, gain_v, routes_v) = local

    def copies_of(index, count, axis, sems, first):
        size = hbm[index].shape[axis] // count
        made = []
        for k in range(count):
            span = pl.ds(size * k, size)
            at = (slice(None), span) if axis else (span, slice(None))
            made.append(
                pltpu.make_async_copy(hbm[index].at[at], local[index].at[at], sems.at[first + k])
            )
        return made

    cuts = 4
    small = {}
    for n, index in enumerate((3, 4, 5, 16, 0, 6, 7, 8, 9, 10, 13, 14, 15)):
        small[index] = copies_of(index, 1, 0, small_sems, n)[0]
    state = [copies_of(1, cuts, 1, state_sems, 0), copies_of(2, cuts, 1, state_sems, cuts)]
    glu_cuts = glu_sems.shape[0] // 2
    value = copies_of(11, glu_cuts, 1, glu_sems, 0)
    gate = copies_of(12, glu_cuts, 1, glu_sems, glu_cuts)
    for index in (3, 4, 5, 16, 0, 6, 7, 8, 9, 10):
        small[index].start()
    for j in range(cuts):
        state[0][j].start()
        state[1][j].start()
    for n in range(glu_cuts):
        value[n].start()
        gate[n].start()
    for index in (13, 14, 15):
        small[index].start()

    seq = u_v.shape[0]
    groups, states = decay_v.shape
    packed = 4
    wide = packed * states
    cols = u_v.shape[1] // cuts
    chans = cols // (groups // cuts)

    small[16].wait()
    code = spread_rows(route_code(routes_v[...]))
    select[...] = jnp.where(code == slot_of_row(code.shape), 1.0, 0.0).astype(bf16)

    small[5].wait()
    small[3].wait()
    small[4].wait()
    pick = iota((groups, groups), 1) == iota((groups, groups), 0)
    step_size = jnp.exp(jnp.sum(jnp.where(pick, log_v[...], 0.0), axis=1, keepdims=True))
    decay = decay_v[...]
    freq = freq_v[...]
    magnitude = jnp.exp(-decay * step_size)
    sin_x, cos_x = sin_cos(freq * step_size)
    a_re = magnitude * cos_x
    a_im = magnitude * sin_x
    lam = -decay
    den = lam * lam + freq * freq
    num = a_re - 1.0
    k_re = (num * lam + a_im * freq) / den
    k_im = (a_im * lam - num * freq) / den
    own = iota((groups, wide), 0) % packed == iota((groups, wide), 1) // states

    def tiled(x):
        twice = jnp.concatenate([x, x], axis=1)
        return jnp.concatenate([twice] * (packed // 2), axis=1)

    def flat(x):
        x = jnp.where(own, tiled(x), 0.0)
        return [
            jnp.sum(x[packed * b : packed * (b + 1)], axis=0, keepdims=True)
            for b in range(groups // packed)
        ]

    a_re, a_im, k_re, k_im = flat(a_re), flat(a_im), flat(k_re), flat(k_im)

    patch = (iota((cols, wide), 0) // chans) % packed == iota((cols, wide), 1) // states

    def weights(ref, j):
        x = ref[cols * j : cols * (j + 1), :].astype(f32)
        return jnp.where(patch, tiled(x), 0.0).astype(bf16)

    lane = iota((seq, cols), 1) // (cols // packed)
    for index in (0, 6, 7):
        small[index].wait()
    for j in range(cuts):
        u = u_v[:, cols * j : cols * (j + 1)].astype(f32)
        spread = jnp.concatenate(
            [jnp.where(lane == k, u, 0.0) for k in range(packed)], axis=0
        ).astype(bf16)
        force_re[j] = dot(spread, weights(inr, j))
        force_im[j] = dot(spread, weights(ini, j))
    for index in (8, 9, 10):
        small[index].wait()
    for j in range(cuts):
        read_re[j] = weights(cr, j)
        read_im[j] = weights(ci, j)

    outs = []
    acts = []
    for j in range(cuts):
        u = u_v[:, cols * j : cols * (j + 1)].astype(f32)
        f_re = force_re[j]
        f_im = force_im[j]
        state[0][j].wait()
        state[1][j].wait()
        fresh_re, fresh_im = [], []
        for k in range(packed):
            b = packed * j + k
            at = slice(wide * b, wide * (b + 1))
            r = slice(seq * k, seq * (k + 1))
            old_re = sr[:, at]
            old_im = si[:, at]
            new_re = a_re[b] * old_re - a_im[b] * old_im + (k_re[b] * f_re[r] - k_im[b] * f_im[r])
            new_im = a_re[b] * old_im + a_im[b] * old_re + (k_re[b] * f_im[r] + k_im[b] * f_re[r])
            nr[:, at] = new_re
            ni[:, at] = new_im
            fresh_re.append(new_re)
            fresh_im.append(new_im)
        for n, (src, dst) in enumerate(((nr, nr_ref), (ni, ni_ref))):
            at = (slice(None), pl.ds(packed * wide * j, packed * wide))
            copy = pltpu.make_async_copy(src.at[at], dst.at[at], out_sems.at[cuts * n + j])
            outs.append(copy)

        def read(parts, ref):
            pairs = [split(x) for x in parts]
            rows = jnp.concatenate([p[0] for p in pairs] + [p[1] for p in pairs], axis=0)
            got = lax.dot_general(
                rows, ref[j], (((1,), (1,)), ((), ())), preferred_element_type=f32
            )
            return got[: packed * seq] + got[packed * seq :]

        both = read(fresh_re, read_re) - read(fresh_im, read_im)
        readout = both[:seq]
        for k in range(1, packed):
            readout = jnp.where(lane == k, both[seq * k : seq * (k + 1)], readout)
        mixed = readout + skip_v[:, cols * j : cols * (j + 1)] * u
        acts.append(jax.nn.gelu(mixed).astype(bf16))

    act = jnp.concatenate(acts, axis=1)
    piece = gv.shape[1] // glu_cuts
    pieces = []
    for n in range(glu_cuts):
        at = slice(piece * n, piece * (n + 1))
        value[n].wait()
        value_part = dot(act, gv[:, at])
        gate[n].wait()
        if n == glu_cuts - 1:
            for copy in outs:
                copy.start()
        pieces.append(value_part * jax.nn.sigmoid(dot(act, gg[:, at])))
    branch = jnp.concatenate(pieces, axis=1)
    for index in (13, 14, 15):
        small[index].wait()
    mid = (res_v[...].astype(f32) + branch * rms_scale(branch) * mix_v[...]).astype(bf16)
    mid_ref[...] = mid
    mid = mid.astype(f32)
    normed = (mid * rms_scale(mid) * gain_v[...]).astype(bf16)
    normed_ref[...] = normed
    width = 512
    for n in range(normed.shape[1] // width):
        at = slice(width * n, width * (n + 1))
        rows = dot(select[...], normed[:, at]).astype(bf16)
        out_ref[:, :, at] = rows.reshape(EXPERTS, CAPACITY, width)
    for copy in outs:
        copy.wait()


def in_hbm(x):
    return pltpu.with_memory_space_constraint(x, pltpu.HBM)


def in_vmem():
    return pl.BlockSpec(memory_space=pltpu.VMEM)


def run_mixer(*operands):
    seq, model = operands[13].shape
    state = operands[1].shape
    return pl.pallas_call(
        mixer_kernel,
        in_specs=[pl.BlockSpec(memory_space=pltpu.HBM)] * MIXER_INS,
        out_specs=[pl.BlockSpec(memory_space=pltpu.HBM)] * 2 + [in_vmem()] * 3,
        out_shape=[
            pltpu.HBM(state, f32),
            pltpu.HBM(state, f32),
            jax.ShapeDtypeStruct((seq, model), bf16),
            jax.ShapeDtypeStruct((seq, model), bf16),
            jax.ShapeDtypeStruct((EXPERTS, CAPACITY, model), bf16),
        ],
        scratch_shapes=[pltpu.VMEM(x.shape, x.dtype) for x in operands]
        + [
            pltpu.VMEM(state, f32),
            pltpu.VMEM(state, f32),
            pltpu.VMEM((EXPERTS * CAPACITY, seq), bf16),
            pltpu.VMEM((4, 256, 256), f32),
            pltpu.VMEM((4, 256, 256), f32),
            pltpu.VMEM((4, 256, 256), bf16),
            pltpu.VMEM((4, 256, 256), bf16),
            pltpu.SemaphoreType.DMA((13,)),
            pltpu.SemaphoreType.DMA((8,)),
            pltpu.SemaphoreType.DMA((2,)),
            pltpu.SemaphoreType.DMA((8,)),
        ],
        compiler_params=pltpu.CompilerParams(vmem_limit_bytes=28 << 20),
        name="mixer",
    )(*map(in_hbm, operands))


def expert_kernel(y_ref, wg_ref, wu_ref, wd_ref, z_ref, h_ref):
    senders, slots, model = y_ref.shape
    x = y_ref[...].reshape(senders * slots, model)
    gate = dot(x, wg_ref[...])
    up = dot(x, wu_ref[...])
    h_ref[...] = (gate * jax.nn.sigmoid(gate) * up).astype(bf16)
    width = 512
    for n in range(model // width):
        at = slice(width * n, width * (n + 1))
        out = dot(h_ref[...], wd_ref[:, at]).astype(bf16)
        z_ref[:, :, at] = out.reshape(senders, slots, width)


def run_expert(y, wg, wu, wd):
    rows = y.shape[0] * y.shape[1]
    return pl.pallas_call(
        expert_kernel,
        in_specs=[in_vmem()] * 4,
        out_specs=in_vmem(),
        out_shape=jax.ShapeDtypeStruct(y.shape, bf16),
        scratch_shapes=[pltpu.VMEM((rows, wg.shape[1]), bf16)],
        compiler_params=pltpu.CompilerParams(vmem_limit_bytes=16 << 20),
        name="expert",
    )(y, wg, wu, wd)


def shared_part(normed_ref, wg_ref, wu_ref, wd_ref, routes_ref, weights_ref, out_ref, mix_ref):
    x = normed_ref[...]
    gate = dot(x, wg_ref[...])
    up = dot(x, wu_ref[...])
    hidden = (gate * jax.nn.sigmoid(gate) * up).astype(bf16)
    out_ref[...] = dot(hidden, wd_ref[...])

    routes = routes_ref[...]
    weights = weights_ref[...]
    top, seq = routes.shape
    code = route_code(routes)
    row = iota(code.shape, 0)
    weight = jnp.zeros(code.shape, f32)
    for k in range(top):
        weight = weight + jnp.where(row == routes[k : k + 1, :], weights[k : k + 1, :], 0.0)
    code = spread_rows(code)
    hit = code == slot_of_row(code.shape)
    hi, lo = split(weight)
    for h, w in enumerate((hi, lo)):
        mix_ref[seq * h : seq * (h + 1), :] = jnp.where(hit, spread_rows(w), 0.0).T.astype(bf16)


def combine_kernel(
    z_ref, normed_ref, sg_ref, su_ref, sd_ref, routes_ref, weights_ref, mid_ref, gain_ref,
    out_ref, shared_ref, mix_ref,
):
    shared_part(
        normed_ref, sg_ref, su_ref, sd_ref, routes_ref, weights_ref, shared_ref, mix_ref
    )
    seq = mid_ref.shape[0]
    both = dot(mix_ref[...], z_ref[...].reshape(mix_ref.shape[1], out_ref.shape[1]))
    routed = both[:seq] + both[seq:]
    combined = shared_ref[...] + routed
    out_ref[...] = (
        mid_ref[...].astype(f32) + combined * rms_scale(combined) * gain_ref[...]
    ).astype(bf16)


def run_combine(z, normed, sg, su, sd, routes, weights, mid, gain):
    return pl.pallas_call(
        combine_kernel,
        in_specs=[in_vmem()] * 9,
        out_specs=in_vmem(),
        out_shape=jax.ShapeDtypeStruct(mid.shape, bf16),
        scratch_shapes=[
            pltpu.VMEM(mid.shape, f32),
            pltpu.VMEM((2 * mid.shape[0], EXPERTS * CAPACITY), bf16),
        ],
        compiler_params=pltpu.CompilerParams(vmem_limit_bytes=16 << 20),
        name="combine",
    )(z, normed, sg, su, sd, routes, weights, mid, gain)


def per_device(
    residual, branch_in, state_real, state_imag, decay_rate, frequency, log_step, input_real,
    input_imag, output_matrix_real, output_matrix_imaginary, skip_gain, glu_value, glu_gate,
    mix_gain, moe_in_gain, moe_out_gain, routes, route_weights, expert_gate, expert_up,
    expert_down, shared_gate, shared_up, shared_down,
):
    states = decay_rate.shape[1]
    row = lambda v: v.reshape(1, -1)
    inr = jnp.transpose(input_real, (0, 2, 1)).reshape(-1, states)
    ini = jnp.transpose(input_imag, (0, 2, 1)).reshape(-1, states)
    cr = output_matrix_real.reshape(-1, states)
    ci = output_matrix_imaginary.reshape(-1, states)
    routes_t = routes.T
    weights_t = route_weights.T
    next_real, next_imag, mid, normed, outgoing = run_mixer(
        branch_in, state_real, state_imag, decay_rate, frequency, row(log_step), inr, ini, cr, ci,
        row(skip_gain), glu_value, glu_gate, residual, row(mix_gain), row(moe_in_gain), routes_t,
    )

    def exchange(x):
        return lax.all_to_all(x, "ep", split_axis=0, concat_axis=0, tiled=True)

    arrived = exchange(outgoing)
    returned = exchange(run_expert(arrived, expert_gate[0], expert_up[0], expert_down[0]))
    layer_out = run_combine(
        returned, normed, shared_gate, shared_up, shared_down, routes_t, weights_t, mid,
        row(moe_out_gain),
    )
    return layer_out, next_real, next_imag


def solution(mesh):
    rows2 = P("ep", None)
    rows3 = P("ep", None, None)
    return jax.shard_map(
        per_device,
        mesh=mesh,
        in_specs=(rows2,) * 4 + (P(),) * 13 + (rows2,) * 2 + (rows3,) * 3 + (P(),) * 3,
        out_specs=(rows2, rows2, rows2),
        check_vma=False,
    )
```
